32 devices in a mesh: sp: 8 (over z, y), tp: 4 (over x, core).
Axes of the slice: x: 2, y: 2, z: 4, core: 2. Of those that a mesh axis runs over, the one named last changes fastest.
Arguments:
- block_input: bfloat16 [8192, 2048], P('sp'), may hold values from -6 to 6
- value_proj: bfloat16 [2048, 1024], P(None, 'tp'), may hold values from -0.125 to 0.125
- gate_proj: bfloat16 [2048, 1024], P(None, 'tp'), may hold values from -0.125 to 0.125
- conv_taps: float32 [31, 1024], P(None, 'tp'), may hold values from -3 to 3
- norm_gain: float32 [1024], P('tp'), may hold values from 0.1 to 1.9
- out_proj: bfloat16 [2048, 1024], P(None, 'tp'), may hold values from -0.125 to 0.125
- grad_output: bfloat16 [8192, 2048], P('sp'), may hold values from -6 to 6
Outputs:
- input_grad: bfloat16 [8192, 2048], P('sp', 'tp')
- value_grad: float32 [2048, 1024], P('sp', 'tp')
- gate_grad: float32 [2048, 1024], P('sp', 'tp')
- out_grad: float32 [2048, 1024], P('sp', 'tp')
- taps_grad: float32 [31, 1024], P(None, 'tp')
- gain_grad: float32 [1024], P('tp')
The draws below stay inside these ranges and needn't reach their ends.
All inputs are finite; a program needn't handle non-finite values.
Results may differ from the reference program's by a relative error of at most 0.015.
Values may be sent and summed in bfloat16 or wider, within the bound.
A program may use at most 64 MiB of HBM per device.

```python
import jax
import jax.numpy as jnp
from jax import lax

D = 2048
C = 1024
K = 31
TOKENS = 8192
N_TP = 4


def draw_conv_taps(key, part):
    base_key, order_key = jax.random.split(key)
    raw_taps = jnp.clip(jax.random.normal(base_key, (K, C), jnp.float32), -4.0, 4.0)
    group_order = jax.random.permutation(order_key, 8).astype(jnp.float32)
    group_index = jnp.arange(C) * 8 // C
    group_scale = 0.3 * 10.0 ** (group_order[group_index] / 7.0)
    return raw_taps * group_scale[None, :] / jnp.sqrt(jnp.float32(K))


def with_spikes(result, key, source, target, blocks, factor):
    def block_of(dim):
        return (jnp.arange(result.shape[dim]) // (result.shape[dim] // blocks)).reshape((-1,) + (1,) * (result.ndim - 1 - dim))

    one_side = jax.random.permutation(key, blocks)[block_of(target)]
    far = (block_of(target) + blocks // 2) % blocks
    return jnp.where((block_of(source) == one_side) | (block_of(source) == far), factor * result, result)


def block_scale(stream_key, shape, cuts, least, high):
    def one(axis_at, parts):
        heights = jax.random.uniform(jax.random.fold_in(jax.random.fold_in(stream_key, 6), axis_at), (parts,), jnp.float32, least / len(cuts), high / len(cuts))
        return jnp.repeat(jnp.exp(heights), shape[axis_at] // parts).reshape((-1,) + (1,) * (len(shape) - axis_at - 1))

    loudness = one(*cuts[0])
    for cut in cuts[1:]:
        loudness = loudness * one(*cut)
    return loudness


def normal_values(stream_key, dims, spread, reach, cuts=(), dtype=jnp.bfloat16):
    values = spread * jax.random.normal(stream_key, dims, jnp.float32)
    if cuts:
        values = values * block_scale(stream_key, dims, cuts, -0.22, 0.18)
    return jnp.clip(values, -reach, reach).astype(dtype)


def bell_draw_with(rng, shape, deviation, most, pieces, heavy, held_as=jnp.bfloat16):
    entries = deviation * jax.random.normal(rng, shape, jnp.float32)
    if pieces:
        entries = entries * block_scale(rng, shape, pieces, -0.22, 0.18)
    return jnp.clip(with_spikes(entries, jax.random.fold_in(rng, 3), *heavy), -most, most).astype(held_as)


def setup_inputs(seed: int = 0) -> dict:
    keys = jax.random.split(jax.random.key(seed), 8)
    block_input = bell_draw_with(keys[0], (TOKENS, D), 1.0, 6.0, ((0, 8),), (0, 1, 8, 2.0))
    value_proj = normal_values(keys[1], (D, C), D ** -0.5, 0.125, ((1, 4),))
    gate_proj = normal_values(keys[2], (D, C), D ** -0.5, 0.125, ((1, 4),))
    conv_taps = draw_conv_taps(jax.random.fold_in(keys[7], 71), 0)
    norm_gain = jnp.clip(1.0 + 0.18 * jax.random.normal(keys[4], (C,), jnp.float32), 0.1, 1.9)
    out_proj = normal_values(keys[5], (D, C), D ** -0.5, 0.125, ((1, 4),))
    grad_output = bell_draw_with(keys[6], (TOKENS, D), 1.0, 6.0, ((0, 8),), (0, 1, 8, 2.0))
    return dict(block_input=block_input, value_proj=value_proj, gate_proj=gate_proj, conv_taps=conv_taps, norm_gain=norm_gain, out_proj=out_proj, grad_output=grad_output)


norm_floor = 0.1

def reference(block_input, value_proj, gate_proj, conv_taps, norm_gain, out_proj, grad_output):
    value = jnp.dot(block_input, value_proj, preferred_element_type=jnp.float32)
    gate_raw = jnp.dot(block_input, gate_proj, preferred_element_type=jnp.float32)
    sgate = jax.nn.sigmoid(gate_raw)
    mixed = (value * sgate).astype(jnp.bfloat16)
    tap_count = conv_taps.shape[0]
    reach_rows = tap_count - 1
    seq_rows = mixed.shape[0]
    history = jnp.concatenate([jnp.zeros((reach_rows, C), jnp.bfloat16), mixed], axis=0)
    conv_out = jnp.zeros((seq_rows, C), jnp.float32)
    for tap_index in range(tap_count):
        offset = reach_rows - tap_index
        conv_out = conv_out + conv_taps[tap_index] * history[offset:offset + seq_rows].astype(jnp.float32)
    center = lax.optimization_barrier(jnp.sum(conv_out, axis=1)) / C
    squares = lax.optimization_barrier(jnp.sum(conv_out * conv_out, axis=1)) / C
    inverse = lax.rsqrt(squares - center * center + norm_floor)
    normed = (conv_out - center[:, None]) * inverse[:, None]
    scaled = normed * norm_gain
    squash = jax.nn.sigmoid(scaled)
    activated = (scaled * squash).astype(jnp.bfloat16)
    slope = jnp.dot(grad_output, out_proj, preferred_element_type=jnp.float32)
    pre_slope = slope * squash * (1.0 + scaled * (1.0 - squash))
    gain_grad = lax.optimization_barrier(jnp.sum(pre_slope * normed, axis=0))
    norm_slope = pre_slope * norm_gain
    slope_sum = lax.optimization_barrier(jnp.sum(norm_slope, axis=1)) / C
    cross_sum = lax.optimization_barrier(jnp.sum(norm_slope * normed, axis=1)) / C
    conv_slope = inverse[:, None] * (norm_slope - slope_sum[:, None] - normed * cross_sum[:, None])
    taps_list = []
    for tap_index in range(tap_count):
        offset = reach_rows - tap_index
        taps_list.append(lax.optimization_barrier(jnp.sum(conv_slope * history[offset:offset + seq_rows].astype(jnp.float32), axis=0)))
    taps_grad = jnp.stack(taps_list)
    future = jnp.concatenate([conv_slope, jnp.zeros((reach_rows, C), jnp.float32)], axis=0)
    mixed_slope = jnp.zeros((seq_rows, C), jnp.float32)
    for tap_index in range(tap_count):
        mixed_slope = mixed_slope + conv_taps[tap_index] * future[tap_index:tap_index + seq_rows]
    value_slope = (mixed_slope * sgate).astype(jnp.bfloat16)
    gate_slope = (mixed_slope * value * sgate * (1.0 - sgate)).astype(jnp.bfloat16)
    value_grad = jnp.dot(block_input.T, value_slope, preferred_element_type=jnp.float32)
    gate_grad = jnp.dot(block_input.T, gate_slope, preferred_element_type=jnp.float32)
    out_grad = jnp.dot(grad_output.T, activated, preferred_element_type=jnp.float32)
    group_width = C // N_TP
    running = jnp.zeros((seq_rows, D), jnp.float32)
    for group_index in range(N_TP):
        first_col = group_index * group_width
        last_col = first_col + group_width
        partial_value = jnp.dot(value_slope[:, first_col:last_col], value_proj[:, first_col:last_col].T, preferred_element_type=jnp.float32)
        partial_value = partial_value + jnp.dot(gate_slope[:, first_col:last_col], gate_proj[:, first_col:last_col].T, preferred_element_type=jnp.float32)
        rounded = lax.optimization_barrier(partial_value.astype(jnp.bfloat16))
        running = running + rounded.astype(jnp.float32)
    input_grad = running.astype(jnp.bfloat16)
    return (input_grad, value_grad, gate_grad, out_grad, taps_grad, gain_grad)
```

```python
import functools

import jax
import jax.numpy as jnp
from jax import lax
from jax.experimental import pallas as pl
from jax.experimental.pallas import tpu as pltpu
from jax.sharding import PartitionSpec as P

NORM_FLOOR = 0.1
LANES = 128
ROW_BLOCK = 128
MATMUL_ROWS = 256
PAD = 32
F32 = jnp.float32
BF16 = jnp.bfloat16
MESH = pl.DeviceIdType.MESH


def dot_nt(a, b):
    return lax.dot_general(a, b, (((1,), (1,)), ((), ())), preferred_element_type=F32)


def dot_tn(a, b):
    return lax.dot_general(a, b, (((0,), (0,)), ((), ())), preferred_element_type=F32)


def kernel(cfg, bi_hbm, wv_hbm, wg_hbm, taps_ref, gain_ref, wo_hbm, go_hbm,
           ig_ref, wgrad_ref, small_ref,
           bi, wv, wg, wo, go, val, sg, slope, hist, nrm, nsl, fut, act, sl, psl, pw,
           st1, st1r, st2, st2r, gvg, gout, yvg, yout, avg, aout, arvg, arout, bvg, bout, brvg, brout,
           xs, xr, tg, tgy, tgz, tgzr,
           ld_sem, halo_sem, st_send, st_recv, pw_send, pw_recv, sl_send, sl_recv,
           x_send, x_recv, y_send, y_recv, a_send, a_recv, b_send, b_recv, ty_send, ty_recv, tz_send, tz_recv):
    nsp, ntp, ny, nz, nx, chan = cfg
    rows, width = bi.shape
    cl = wv.shape[1]
    groups = cl // LANES
    tap_count = taps_ref.shape[0]
    nb = rows // ROW_BLOCK
    vpb = ROW_BLOCK // 8
    nrc = rows // MATMUL_ROWS
    ds = width // nsp
    dt = width // ntp
    sp = lax.axis_index("sp")
    tp = lax.axis_index("tp")
    z = sp // ny
    y = sp % ny
    x = tp // 2
    core = tp % 2

    def wrap(v, n):
        return lax.rem(v, n)

    loads = {}

    def load(name, src, dst, i):
        c = pltpu.make_async_copy(src, dst, ld_sem.at[i])
        c.start()
        loads[name] = c

    load("wv", wv_hbm, wv, 0)
    load("wg", wg_hbm, wg, 1)
    for n, i in enumerate(reversed(range(nrc))):
        s = pl.ds(i * MATMUL_ROWS, MATMUL_ROWS)
        load("bi%d" % i, bi_hbm.at[s], bi.at[s], 2 + n)
    load("wo", wo_hbm, wo, 2 + nrc)
    load("go", go_hbm, go, 3 + nrc)

    barrier = pltpu.get_barrier_semaphore()
    for o in range(1, nsp):
        pl.semaphore_signal(barrier, inc=1, device_id={"sp": wrap(sp + o, nsp)}, device_id_type=MESH)
    for o in range(1, ntp):
        pl.semaphore_signal(barrier, inc=1, device_id={"tp": wrap(tp + o, ntp)}, device_id_type=MESH)

    def remote(src, dst, ssem, rsem, dev):
        return pltpu.make_async_remote_copy(
            src_ref=src, dst_ref=dst, send_sem=ssem, recv_sem=rsem, device_id=dev, device_id_type=MESH)

    def glu(i):
        r = i * MATMUL_ROWS
        a = bi[r:r + MATMUL_ROWS, :]
        v = jnp.dot(a, wv[...], preferred_element_type=F32)
        s = jax.nn.sigmoid(jnp.dot(a, wg[...], preferred_element_type=F32))
        m = (v * s).astype(BF16).astype(F32)
        for g in range(groups):
            c = slice(g * LANES, (g + 1) * LANES)
            val[g, r:r + MATMUL_ROWS, :] = v[:, c]
            sg[g, r:r + MATMUL_ROWS, :] = s[:, c]
            hist[g, PAD + r:PAD + r + MATMUL_ROWS, :] = m[:, c]

    halo = remote(hist.at[:, pl.ds(rows, PAD), :], hist.at[:, pl.ds(0, PAD), :],
                  halo_sem.at[0], halo_sem.at[1], {"sp": jnp.minimum(sp + 1, nsp - 1)})
    back = remote(fut.at[:, pl.ds(0, PAD), :], fut.at[:, pl.ds(rows, PAD), :],
                  halo_sem.at[2], halo_sem.at[3], {"sp": jnp.maximum(sp - 1, 0)})
    has_next = sp < nsp - 1
    has_prev = sp > 0

    @pl.when(jnp.logical_not(has_prev))
    def _():
        hist[:, 0:PAD, :] = jnp.zeros((groups, PAD, LANES), F32)

    @pl.when(jnp.logical_not(has_next))
    def _():
        fut[:, rows:rows + PAD, :] = jnp.zeros((groups, PAD, LANES), F32)

    loads["wv"].wait()
    loads["wg"].wait()
    partner = {"tp": 2 * x + 1 - core}
    pws = []
    for n, i in enumerate(reversed(range(nrc))):
        loads["bi%d" % i].wait()
        glu(i)
        if n == 0:
            pl.semaphore_wait(barrier, nsp + ntp - 2)

            @pl.when(has_next)
            def _():
                halo.start()

            for xx in range(nx):
                for j, w in enumerate((wv, wg)):
                    first = pl.multiple_of((2 * xx + 1 - core) * dt, dt)
                    c = remote(w.at[pl.ds(first, dt), :], pw.at[xx, j], pw_send.at[xx, j], pw_recv.at[xx, j], partner)
                    c.start()
                    pws.append(c)

    lane = lax.broadcasted_iota(jnp.int32, (8, LANES), 1)

    def pack(packed, red, b):
        for i in range(vpb):
            packed = jnp.where(lane == b * vpb + i, red[8 * i:8 * i + 8], packed)
        return packed

    def unpack(rolled):
        return jnp.concatenate([rolled[:, i:i + 1] for i in range(vpb)], axis=0)

    def roll_to(packed, b):
        return pltpu.roll(packed, lax.rem(LANES - b * vpb, LANES), 1)

    def tap(k, g):
        return taps_ref[k:k + 1, g * LANES:(g + 1) * LANES]

    def conv_block(b, carry):
        psum, psq = carry
        s = q = None
        for g in range(groups):
            acc = jnp.zeros((ROW_BLOCK, LANES), F32)
            for k in range(tap_count):
                acc = acc + tap(k, g) * hist[g, pl.ds(b * ROW_BLOCK + (PAD - k), ROW_BLOCK), :]
            nrm[g, pl.ds(pl.multiple_of(b * ROW_BLOCK, ROW_BLOCK), ROW_BLOCK), :] = acc
            s = acc if s is None else s + acc
            q = acc * acc if q is None else q + acc * acc
        return (pack(psum, jnp.sum(s, axis=1, keepdims=True), b),
                pack(psq, jnp.sum(q, axis=1, keepdims=True), b))

    zero = jnp.zeros((8, LANES), F32)
    carry = lax.fori_loop(0, nb - 1, lambda i, c: conv_block(nb - 1 - i, c), (zero, zero))

    @pl.when(has_prev)
    def _():
        halo.wait_recv()

    psum, psq = conv_block(0, carry)
    st1[0] = psum
    st1[1] = psq

    def share(which, src, dst):
        out = []
        for o in range(1, ntp):
            c = remote(src, dst.at[o - 1], st_send.at[which, o - 1], st_recv.at[which, o - 1],
                       {"tp": wrap(tp + o, ntp)})
            c.start()
            out.append(c)
        return out

    st_copies = share(0, st1, st1r)

    loads["wo"].wait()
    loads["go"].wait()
    for i in range(nrc):
        r = i * MATMUL_ROWS
        t = jnp.dot(go[r:r + MATMUL_ROWS, :], wo[...], preferred_element_type=F32)
        for g in range(groups):
            slope[g, r:r + MATMUL_ROWS, :] = t[:, g * LANES:(g + 1) * LANES]

    for c in st_copies:
        c.wait()
    tsum, tsq = st1[0], st1[1]
    for o in range(ntp - 1):
        tsum = tsum + st1r[o, 0]
        tsq = tsq + st1r[o, 1]
    center = tsum / chan
    inverse = lax.rsqrt(tsq / chan - center * center + NORM_FLOOR)

    def norm_block(b, carry):
        psum, pcross, gacc = carry
        r = pl.ds(pl.multiple_of(b * ROW_BLOCK, ROW_BLOCK), ROW_BLOCK)
        cen = unpack(roll_to(center, b))
        inv = unpack(roll_to(inverse, b))
        s = q = None
        gout_acc = []
        for g in range(groups):
            gain = gain_ref[:, g * LANES:(g + 1) * LANES]
            normed = (nrm[g, r, :] - cen) * inv
            scaled = normed * gain
            squash = jax.nn.sigmoid(scaled)
            act[r, g * LANES:(g + 1) * LANES] = (scaled * squash).astype(BF16)
            pre = slope[g, r, :] * squash * (1.0 + scaled * (1.0 - squash))
            pn = pre * normed
            tot = gacc[g]
            for i in range(vpb):
                tot = tot + pn[8 * i:8 * i + 8]
            gout_acc.append(tot)
            ns = pre * gain
            nrm[g, r, :] = normed
            nsl[g, r, :] = ns * inv
            cross = ns * normed
            s = ns if s is None else s + ns
            q = cross if q is None else q + cross
        return (pack(psum, jnp.sum(s, axis=1, keepdims=True), b),
                pack(pcross, jnp.sum(q, axis=1, keepdims=True), b), tuple(gout_acc))

    psum, pcross, gacc = lax.fori_loop(0, nb, norm_block, (zero, zero, (zero,) * groups))
    st2[0] = psum
    st2[1] = pcross
    st_copies = share(1, st2, st2r)

    per = max(1, min(256, width) // ds)
    zh = z // 2
    zl = z % 2
    nh = nz // 2

    def plane(u):
        side = zl if u % 2 else 1 - zl
        return 2 * wrap(zh + u // 2 + 1, nh) + side

    peers = [(u, r) for u in range(nz) for r in range(1, ny)]

    def y_copies(which, src, dst):
        out = {}
        for o, r in peers:
            yy = wrap(y + r, ny)
            out[o, r] = remote(src.at[plane(o) * ny + yy], dst.at[r - 1, o], y_send.at[which, r - 1, o],
                               y_recv.at[which, r - 1, o], {"sp": z * ny + yy})
        return out

    def weight_chunk(src, right, dst, chunk):
        cols = pl.ds(pl.multiple_of(chunk * per * ds, per * ds), per * ds)
        t = dot_tn(src[:, cols], right[...]).astype(BF16)
        for j in range(per):
            dst[chunk * per + j] = t[j * ds:(j + 1) * ds]

    def weight_peer_part(src, right, dst, copies, send=True):
        if per == 1:
            for o, r in peers:
                weight_chunk(src, right, dst, plane(o) * ny + wrap(y + r, ny))
                if send:
                    copies[o, r].start()
        else:
            for chunk in range(nsp // per):
                weight_chunk(src, right, dst, chunk)
            for o, r in peers:
                if send:
                    copies[o, r].start()

    def weight_own_part(src, right, dst):
        if per == 1:
            for o in range(nz):
                weight_chunk(src, right, dst, plane(o) * ny + y)

    yc_out = y_copies(0, gout, yout)
    yc_vg = y_copies(1, gvg, yvg)
    weight_peer_part(go, act, gout, yc_out, send=False)

    for c in st_copies:
        c.wait()
    tsum, tcross = st2[0], st2[1]
    for o in range(ntp - 1):
        tsum = tsum + st2r[o, 0]
        tcross = tcross + st2r[o, 1]
    tsum = tsum / chan * inverse
    tcross = tcross / chan * inverse

    def slope_block(b, c):
        r = pl.ds(pl.multiple_of(b * ROW_BLOCK, ROW_BLOCK), ROW_BLOCK)
        ss = unpack(roll_to(tsum, b))
        cs = unpack(roll_to(tcross, b))
        for g in range(groups):
            fut[g, r, :] = nsl[g, r, :] - ss - nrm[g, r, :] * cs
        return c

    slope_block(0, 0)

    @pl.when(has_prev)
    def _():
        back.start()

    for o, r in peers:
        yc_out[o, r].start()

    lax.fori_loop(1, nb, slope_block, 0)

    def adjoint_block(b, c):
        r = pl.ds(pl.multiple_of(b * ROW_BLOCK, ROW_BLOCK), ROW_BLOCK)
        for g in range(groups):
            acc = jnp.zeros((ROW_BLOCK, LANES), F32)
            for k in range(tap_count):
                acc = acc + tap(k, g) * fut[g, pl.ds(b * ROW_BLOCK + k, ROW_BLOCK), :]
            s = sg[g, r, :]
            t = acc * s
            sl[r, g * LANES:(g + 1) * LANES] = t.astype(BF16)
            sl[r, cl + g * LANES:cl + (g + 1) * LANES] = (t * val[g, r, :] * (1.0 - s)).astype(BF16)
        return c

    def input_part(i, xx):
        r = slice(i * MATMUL_ROWS, (i + 1) * MATMUL_ROWS)
        blk = pl.ds(pl.multiple_of((2 * xx + core) * dt, dt), dt)
        t = dot_nt(sl[r, 0:cl], wv[blk, :]) + dot_nt(sl[r, cl:2 * cl], wg[blk, :])
        return t + dot_nt(psl[r, 0:cl], pw[xx, 0]) + dot_nt(psl[r, cl:2 * cl], pw[xx, 1])

    xc = []

    def input_send(i):
        slc[i].wait()
        for o in range(1, nx):
            xx = wrap(x + o, nx)
            xs[o - 1, i] = input_part(i, xx).astype(BF16)
            c = remote(xs.at[o - 1, i], xr.at[o - 1, i], x_send.at[o - 1, i], x_recv.at[o - 1, i],
                       {"tp": 2 * xx + core})
            c.start()
            xc.append(c)

    for c in pws:
        c.wait()
    bpc = MATMUL_ROWS // ROW_BLOCK
    slc = []
    for i in range(nrc):
        if i == nrc - 1:
            lax.fori_loop(i * bpc, nb - 1, adjoint_block, 0)

            @pl.when(has_next)
            def _():
                back.wait_recv()

            adjoint_block(nb - 1, 0)
        else:
            lax.fori_loop(i * bpc, (i + 1) * bpc, adjoint_block, 0)
        s = pl.ds(i * MATMUL_ROWS, MATMUL_ROWS)
        c = remote(sl.at[s], psl.at[s], sl_send.at[i], sl_recv.at[i], partner)
        c.start()
        slc.append(c)
        if i > 0:
            input_send(i - 1)

    weight_peer_part(bi, sl, gvg, yc_vg)
    input_send(nrc - 1)

    weight_own_part(go, act, gout)
    weight_own_part(bi, sl, gvg)

    def y_sum(u, gb, yb, ycs):
        t = gb[plane(u) * ny + y].astype(F32)
        for r in range(1, ny):
            ycs[u, r].wait()
            t = t + yb[r - 1, u].astype(F32)
        return t

    pair = {"sp": (2 * zh + 1 - zl) * ny + y}
    across = {}

    def a_step(which, h):
        gb, yb, ycs, buf, rbuf = ((gout, yout, yc_out, aout, arout), (gvg, yvg, yc_vg, avg, arvg))[which]
        buf[h] = y_sum(2 * h, gb, yb, ycs).astype(BF16)
        c = remote(buf.at[h], rbuf.at[h], a_send.at[which, h], a_recv.at[which, h], pair)
        c.start()
        across[which, h] = c

    def b_sum(which, h):
        gb, yb, ycs, rbuf = ((gout, yout, yc_out, arout), (gvg, yvg, yc_vg, arvg))[which]
        t = y_sum(2 * h + 1, gb, yb, ycs)
        across[which, h].wait()
        return t + rbuf[h].astype(F32)

    b_copies = {}

    def b_step(which, h):
        buf, rbuf = ((bout, brout), (bvg, brvg))[which]
        buf[h] = b_sum(which, h).astype(BF16)
        c = remote(buf.at[h], rbuf.at[h], b_send.at[which, h], b_recv.at[which, h],
                   {"sp": (2 * wrap(zh + h + 1, nh) + zl) * ny + y})
        c.start()
        b_copies[which, h] = c

    def final_sum(which):
        rbuf = (brout, brvg)[which]
        t = b_sum(which, nh - 1)
        for h in range(nh - 1):
            b_copies[which, h].wait()
            t = t + rbuf[h].astype(F32)
        return t

    for h in range(nh):
        a_step(0, h)

    step = 4
    for g in range(groups):
        def tap_block(b, accs, g=g):
            r = b * 8 * step
            f = fut[g, pl.ds(pl.multiple_of(r, 8 * step), 8 * step), :]
            out = []
            for k in range(tap_count):
                p = f * hist[g, pl.ds(r + (PAD - k), 8 * step), :]
                t = accs[k]
                for i in range(step):
                    t = t + p[8 * i:8 * i + 8]
                out.append(t)
            return tuple(out)

        accs = lax.fori_loop(0, rows // (8 * step), tap_block, (zero,) * tap_count)
        for k in range(tap_count):
            tg[k:k + 1, g * LANES:(g + 1) * LANES] = jnp.sum(accs[k], axis=0, keepdims=True)
        tg[tap_count:tap_count + 1, g * LANES:(g + 1) * LANES] = jnp.sum(gacc[g], axis=0, keepdims=True)

    tzc = []
    for o in range(1, nz):
        c = remote(tg, tgzr.at[o - 1], tz_send.at[o - 1], tz_recv.at[o - 1], {"sp": wrap(z + o, nz) * ny + y})
        c.start()
        tzc.append(c)

    for h in range(nh - 1):
        b_step(0, h)
    a_step(1, 0)
    t = tg[...]
    for o in range(1, nz):
        tzc[o - 1].wait()
        t = t + tgzr[o - 1]
    tgz[...] = t
    tyc = []
    for r in range(1, ny):
        c = remote(tgz, tgy.at[r - 1], ty_send.at[r - 1], ty_recv.at[r - 1], {"sp": z * ny + wrap(y + r, ny)})
        c.start()
        tyc.append(c)
    for h in range(nh - 1):
        b_step(1, h)
        a_step(1, h + 1)

    wgrad_ref[2] = final_sum(0)

    for i in range(nrc):
        t = input_part(i, x)
        for o in range(1, nx):
            xc[i * (nx - 1) + o - 1].wait()
            t = t + xr[o - 1, i].astype(F32)
        ig_ref[i * MATMUL_ROWS:(i + 1) * MATMUL_ROWS, :] = t.astype(BF16)


    own = final_sum(1)
    wgrad_ref[0] = own[:, 0:cl]
    wgrad_ref[1] = own[:, cl:2 * cl]

    t = tgz[...]
    for r in range(1, ny):
        tyc[r - 1].wait()
        t = t + tgy[r - 1]
    small_ref[...] = t

    @pl.when(has_next)
    def _():
        halo.wait_send()

    @pl.when(has_prev)
    def _():
        back.wait_send()


def hand_out(ig_in, wgrad_in, small_in, ig_ref, vgrad_ref, ggrad_ref, ograd_ref, tgrad_ref, gaingrad_ref,
             ig, wgrad, small, taps, gain, in_sem, out_sem):
    tap_count = tgrad_ref.shape[0]
    parts = ig.shape[0] // MATMUL_ROWS
    moves = [(small_in, small, ((taps, tgrad_ref), (gain, gaingrad_ref)))]
    for i in range(parts):
        s = pl.ds(i * MATMUL_ROWS, MATMUL_ROWS)
        moves.append((ig_in.at[s], ig.at[s], ((ig.at[s], ig_ref.at[s]),)))
    for i, ref in enumerate((vgrad_ref, ggrad_ref, ograd_ref)):
        moves.append((wgrad_in.at[i], wgrad.at[i], ((wgrad.at[i], ref),)))
    ins = [pltpu.make_async_copy(src, dst, in_sem.at[i]) for i, (src, dst, _) in enumerate(moves)]
    for c in ins:
        c.start()
    outs = []
    for c, (_, _, stores) in zip(ins, moves):
        c.wait()
        if len(stores) == 2:
            taps[...] = small[0:tap_count]
            gain[...] = small[tap_count:tap_count + 1]
        for src, dst in stores:
            outs.append(pltpu.make_async_copy(src, dst, out_sem.at[len(outs)]))
            outs[-1].start()
    for c in outs:
        c.wait()


def shards(nsp, ntp, block_input, value_proj, gate_proj, conv_taps, norm_gain, out_proj, grad_output):
    rows, width = block_input.shape
    cl = value_proj.shape[1]
    chan = cl * ntp
    nx = ntp // 2
    ny = nx
    nz = nsp // ny
    nh = nz // 2
    nb_slots = max(nh - 1, 1)
    groups = cl // LANES
    ds = width // nsp
    dt = width // ntp
    nrc = rows // MATMUL_ROWS
    tap_count = conv_taps.shape[0]
    dma = pltpu.SemaphoreType.DMA
    vm = pltpu.VMEM
    wide = vm((groups, rows, LANES), F32)
    padded = vm((groups, rows + PAD, LANES), F32)
    tpad = -(-(tap_count + 1) // 8) * 8
    any_spec = pl.BlockSpec(memory_space=pltpu.HBM)
    vmem_spec = pl.BlockSpec(memory_space=pltpu.VMEM)
    outs = pl.pallas_call(
        functools.partial(kernel, (nsp, ntp, ny, nz, nx, float(chan))),
        out_shape=(
            jax.ShapeDtypeStruct((rows, dt), BF16),
            jax.ShapeDtypeStruct((3, ds, cl), F32),
            jax.ShapeDtypeStruct((tpad, cl), F32),
        ),
        in_specs=[any_spec, any_spec, any_spec, vmem_spec, vmem_spec, any_spec, any_spec],
        out_specs=[vmem_spec] * 3,
        scratch_shapes=[
            vm((rows, width), BF16), vm((width, cl), BF16), vm((width, cl), BF16), vm((width, cl), BF16),
            vm((rows, width), BF16),
            wide, wide, wide, padded, wide, wide, padded,
            vm((rows, cl), BF16), vm((rows, 2 * cl), BF16), vm((rows, 2 * cl), BF16),
            vm((nx, 2, dt, cl), BF16),
            vm((2, 8, LANES), F32), vm((ntp - 1, 2, 8, LANES), F32),
            vm((2, 8, LANES), F32), vm((ntp - 1, 2, 8, LANES), F32),
            vm((nsp, ds, 2 * cl), BF16), vm((nsp, ds, cl), BF16),
            vm((ny - 1, nz, ds, 2 * cl), BF16), vm((ny - 1, nz, ds, cl), BF16),
            vm((nh, ds, 2 * cl), BF16), vm((nh, ds, cl), BF16),
            vm((nh, ds, 2 * cl), BF16), vm((nh, ds, cl), BF16),
            vm((nb_slots, ds, 2 * cl), BF16), vm((nb_slots, ds, cl), BF16),
            vm((nb_slots, ds, 2 * cl), BF16), vm((nb_slots, ds, cl), BF16),
            vm((nx - 1, nrc, MATMUL_ROWS, dt), BF16), vm((nx - 1, nrc, MATMUL_ROWS, dt), BF16),
            vm((tpad, cl), F32), vm((ny - 1, tpad, cl), F32),
            vm((tpad, cl), F32), vm((nz - 1, tpad, cl), F32),
            dma((4 + nrc,)), dma((4,)),
            dma((2, ntp - 1)), dma((2, ntp - 1)),
            dma((nx, 2)), dma((nx, 2)),
            dma((nrc,)), dma((nrc,)),
            dma((nx - 1, nrc)), dma((nx - 1, nrc)),
            dma((2, ny - 1, nz)), dma((2, ny - 1, nz)),
            dma((2, nh)), dma((2, nh)),
            dma((2, nb_slots)), dma((2, nb_slots)),
            dma((ny - 1,)), dma((ny - 1,)),
            dma((nz - 1,)), dma((nz - 1,)),
        ],
        compiler_params=pltpu.CompilerParams(
            collective_id=0, has_side_effects=True, vmem_limit_bytes=60 * 1000 * 1000),
    )(block_input, value_proj, gate_proj, conv_taps, norm_gain.reshape(1, cl), out_proj, grad_output)
    outs = pl.pallas_call(
        hand_out,
        out_shape=(
            jax.ShapeDtypeStruct((rows, dt), BF16),
            jax.ShapeDtypeStruct((ds, cl), F32),
            jax.ShapeDtypeStruct((ds, cl), F32),
            jax.ShapeDtypeStruct((ds, cl), F32),
            jax.ShapeDtypeStruct((tap_count, cl), F32),
            jax.ShapeDtypeStruct((1, cl), F32),
        ),
        in_specs=[any_spec] * 3,
        out_specs=[any_spec] * 6,
        scratch_shapes=[
            vm((rows, dt), BF16), vm((3, ds, cl), F32), vm((tpad, cl), F32),
            vm((tap_count, cl), F32), vm((1, cl), F32),
            dma((4 + nrc,)), dma((5 + nrc,)),
        ],
        compiler_params=pltpu.CompilerParams(vmem_limit_bytes=60 * 1000 * 1000),
    )(*outs)
    return outs[:5] + (outs[5].reshape(cl),)


def solution(mesh):
    return jax.shard_map(
        functools.partial(shards, mesh.shape["sp"], mesh.shape["tp"]),
        mesh=mesh,
        in_specs=(
            P("sp", None),
            P(None, "tp"),
            P(None, "tp"),
            P(None, "tp"),
            P("tp"),
            P(None, "tp"),
            P("sp", None),
        ),
        out_specs=(
            P("sp", "tp"),
            P("sp", "tp"),
            P("sp", "tp"),
            P("sp", "tp"),
            P(None, "tp"),
            P("tp"),
        ),
        check_vma=False,
    )
```

```python
import functools

import jax
import jax.numpy as jnp
from jax import lax
from jax.experimental import pallas as pl
from jax.experimental.pallas import tpu as pltpu
from jax.sharding import PartitionSpec as P

NORM_FLOOR = 0.1
LANES = 128
ROW_BLOCK = 128
MATMUL_ROWS = 256
PAD = 32
F32 = jnp.float32
BF16 = jnp.bfloat16
MESH = pl.DeviceIdType.MESH


def dot_nt(a, b):
    return lax.dot_general(a, b, (((1,), (1,)), ((), ())), preferred_element_type=F32)


def dot_tn(a, b):
    return lax.dot_general(a, b, (((0,), (0,)), ((), ())), preferred_element_type=F32)


def kernel(cfg, bi_hbm, wv_hbm, wg_hbm, taps_hbm, gain_hbm, wo_hbm, go_hbm,
           ig_ref, wgrad_ref, tgrad_ref, gaingrad_ref,
           bi, wv, wg, wo, go, taps_ref, gain_ref, val, sg, slope, hist, nrm, nsl, fut, act, sl, psl, pw,
           st1, st1r, st2, st2r, spa, spb, gb, yb, ab, ar, bb, br,
           xs, xr, tg, tgy, tgz, tgzr,
           ld_sem, halo_sem, st_send, st_recv, pw_send, pw_recv, sl_send, sl_recv,
           x_send, x_recv, y_send, y_recv, a_send, a_recv, b_send, b_recv, ty_send, ty_recv, tz_send, tz_recv):
    nsp, ntp, ny, nz, nx, chan = cfg
    rows, width = bi.shape
    cl = wv.shape[1]
    groups = cl // LANES
    tap_count = taps_ref.shape[0]
    nb = rows // ROW_BLOCK
    vpb = ROW_BLOCK // 8
    nrc = rows // MATMUL_ROWS
    ds = width // nsp
    dt = width // ntp
    sp = lax.axis_index("sp")
    tp = lax.axis_index("tp")
    z = sp // ny
    y = sp % ny
    x = tp // 2
    core = tp % 2

    def wrap(v, n):
        return lax.rem(v, n)

    loads = {}

    def load(name, src, dst, i):
        c = pltpu.make_async_copy(src, dst, ld_sem.at[i])
        c.start()
        loads[name] = c

    load("wv", wv_hbm, wv, 0)
    load("wg", wg_hbm, wg, 1)
    for n, i in enumerate(reversed(range(nrc))):
        s = pl.ds(i * MATMUL_ROWS, MATMUL_ROWS)
        load("bi%d" % i, bi_hbm.at[s], bi.at[s], 2 + n)
    load("taps", taps_hbm, taps_ref, 2 + nrc)
    load("gain", gain_hbm, gain_ref, 3 + nrc)
    load("wo", wo_hbm, wo, 4 + nrc)
    load("go", go_hbm, go, 5 + nrc)

    barrier = pltpu.get_barrier_semaphore()
    for o in range(1, nsp):
        pl.semaphore_signal(barrier, inc=1, device_id={"sp": wrap(sp + o, nsp)}, device_id_type=MESH)
    for o in range(1, ntp):
        pl.semaphore_signal(barrier, inc=1, device_id={"tp": wrap(tp + o, ntp)}, device_id_type=MESH)

    def remote(src, dst, ssem, rsem, dev):
        return pltpu.make_async_remote_copy(
            src_ref=src, dst_ref=dst, send_sem=ssem, recv_sem=rsem, device_id=dev, device_id_type=MESH)

    def glu(i):
        r = i * MATMUL_ROWS
        a = bi[r:r + MATMUL_ROWS, :]
        v = jnp.dot(a, wv[...], preferred_element_type=F32)
        s = jax.nn.sigmoid(jnp.dot(a, wg[...], preferred_element_type=F32))
        m = (v * s).astype(BF16).astype(F32)
        for g in range(groups):
            c = slice(g * LANES, (g + 1) * LANES)
            val[g, r:r + MATMUL_ROWS, :] = v[:, c]
            sg[g, r:r + MATMUL_ROWS, :] = s[:, c]
            hist[g, PAD + r:PAD + r + MATMUL_ROWS, :] = m[:, c]

    halo = remote(hist.at[:, pl.ds(rows, PAD), :], hist.at[:, pl.ds(0, PAD), :],
                  halo_sem.at[0], halo_sem.at[1], {"sp": jnp.minimum(sp + 1, nsp - 1)})
    back = remote(fut.at[:, pl.ds(0, PAD), :], fut.at[:, pl.ds(rows, PAD), :],
                  halo_sem.at[2], halo_sem.at[3], {"sp": jnp.maximum(sp - 1, 0)})
    has_next = sp < nsp - 1
    has_prev = sp > 0

    @pl.when(jnp.logical_not(has_prev))
    def _():
        hist[:, 0:PAD, :] = jnp.zeros((groups, PAD, LANES), F32)

    @pl.when(jnp.logical_not(has_next))
    def _():
        fut[:, rows:rows + PAD, :] = jnp.zeros((groups, PAD, LANES), F32)

    loads["wv"].wait()
    loads["wg"].wait()
    partner = {"tp": 2 * x + 1 - core}
    pws = []
    for n, i in enumerate(reversed(range(nrc))):
        loads["bi%d" % i].wait()
        glu(i)
        if n == 0:
            pl.semaphore_wait(barrier, nsp + ntp - 2)

            @pl.when(has_next)
            def _():
                halo.start()

            for xx in range(nx):
                for j, w in enumerate((wv, wg)):
                    first = pl.multiple_of((2 * xx + 1 - core) * dt, dt)
                    c = remote(w.at[pl.ds(first, dt), :], pw.at[xx, j], pw_send.at[xx, j], pw_recv.at[xx, j], partner)
                    c.start()
                    pws.append(c)

    lane = lax.broadcasted_iota(jnp.int32, (8, LANES), 1)

    def pack(packed, red, b):
        for i in range(vpb):
            packed = jnp.where(lane == b * vpb + i, red[8 * i:8 * i + 8], packed)
        return packed

    ahead = (lax.broadcasted_iota(jnp.int32, (ROW_BLOCK, LANES), 1)
             - lax.broadcasted_iota(jnp.int32, (ROW_BLOCK, LANES), 0) // 8)
    ones = jnp.ones((3 * LANES, LANES), BF16)

    def spread(packed, dst):
        high = packed.astype(BF16).astype(F32)
        rest = packed - high
        mid = rest.astype(BF16).astype(F32)
        parts = [jnp.concatenate([p] * vpb, axis=0) for p in (high, mid, rest - mid)]
        for b in range(nb):
            own = ahead == b * vpb
            t = jnp.concatenate([jnp.where(own, p, 0.0).astype(BF16) for p in parts], axis=1)
            dst[b * ROW_BLOCK:(b + 1) * ROW_BLOCK, :] = jnp.dot(t, ones, preferred_element_type=F32)

    def tap(k, g):
        return taps_ref[k:k + 1, g * LANES:(g + 1) * LANES]

    def conv_block(b, carry):
        psum, psq = carry
        s = q = None
        for g in range(groups):
            acc = jnp.zeros((ROW_BLOCK, LANES), F32)
            for k in range(tap_count):
                acc = acc + tap(k, g) * hist[g, pl.ds(b * ROW_BLOCK + (PAD - k), ROW_BLOCK), :]
            nrm[g, pl.ds(pl.multiple_of(b * ROW_BLOCK, ROW_BLOCK), ROW_BLOCK), :] = acc
            s = acc if s is None else s + acc
            q = acc * acc if q is None else q + acc * acc
        return (pack(psum, jnp.sum(s, axis=1, keepdims=True), b),
                pack(psq, jnp.sum(q, axis=1, keepdims=True), b))

    zero = jnp.zeros((8, LANES), F32)
    loads["taps"].wait()
    loads["gain"].wait()
    carry = lax.fori_loop(0, nb - 1, lambda i, c: conv_block(nb - 1 - i, c), (zero, zero))

    @pl.when(has_prev)
    def _():
        halo.wait_recv()

    psum, psq = conv_block(0, carry)
    st1[0] = psum
    st1[1] = psq

    def share(which, src, dst):
        out = []
        for o in range(1, ntp):
            c = remote(src, dst.at[o - 1], st_send.at[which, o - 1], st_recv.at[which, o - 1],
                       {"tp": wrap(tp + o, ntp)})
            c.start()
            out.append(c)
        return out

    st_copies = share(0, st1, st1r)

    loads["wo"].wait()
    loads["go"].wait()
    for i in range(nrc):
        r = i * MATMUL_ROWS
        t = jnp.dot(go[r:r + MATMUL_ROWS, :], wo[...], preferred_element_type=F32)
        for g in range(groups):
            slope[g, r:r + MATMUL_ROWS, :] = t[:, g * LANES:(g + 1) * LANES]

    for c in st_copies:
        c.wait()
    tsum, tsq = st1[0], st1[1]
    for o in range(ntp - 1):
        tsum = tsum + st1r[o, 0]
        tsq = tsq + st1r[o, 1]
    center = tsum / chan
    inverse = lax.rsqrt(tsq / chan - center * center + NORM_FLOOR)

    spread(center, spa)
    spread(inverse, spb)

    def norm_block(b, carry):
        psum, pcross, gacc = carry
        r = pl.ds(pl.multiple_of(b * ROW_BLOCK, ROW_BLOCK), ROW_BLOCK)
        cen = spa[r, :]
        inv = spb[r, :]
        s = q = None
        gout_acc = []
        for g in range(groups):
            gain = gain_ref[:, g * LANES:(g + 1) * LANES]
            normed = (nrm[g, r, :] - cen) * inv
            scaled = normed * gain
            squash = jax.nn.sigmoid(scaled)
            act[r, g * LANES:(g + 1) * LANES] = (scaled * squash).astype(BF16)
            pre = slope[g, r, :] * squash * (1.0 + scaled * (1.0 - squash))
            pn = pre * normed
            tot = gacc[g]
            for i in range(vpb):
                tot = tot + pn[8 * i:8 * i + 8]
            gout_acc.append(tot)
            ns = pre * gain
            nrm[g, r, :] = normed
            nsl[g, r, :] = ns * inv
            cross = ns * normed
            s = ns if s is None else s + ns
            q = cross if q is None else q + cross
        return (pack(psum, jnp.sum(s, axis=1, keepdims=True), b),
                pack(pcross, jnp.sum(q, axis=1, keepdims=True), b), tuple(gout_acc))

    psum, pcross, gacc = lax.fori_loop(0, nb, norm_block, (zero, zero, (zero,) * groups))
    st2[0] = psum
    st2[1] = pcross
    st_copies = share(1, st2, st2r)

    per = max(1, min(256, width) // ds)
    zh = z // 2
    zl = z % 2
    nh = nz // 2

    def plane(u):
        side = zl if u % 2 else 1 - zl
        return 2 * wrap(zh + u // 2 + 1, nh) + side

    peers = [(u, r) for u in range(nz) for r in range(1, ny)]

    y_copies = {}
    for which in range(3):
        for o, r in peers:
            yy = wrap(y + r, ny)
            y_copies[which, o, r] = remote(gb.at[which, plane(o) * ny + yy], yb.at[which, r - 1, o],
                                           y_send.at[which, r - 1, o], y_recv.at[which, r - 1, o],
                                           {"sp": z * ny + yy})

    def y_start(which, o):
        for r in range(1, ny):
            y_copies[which, o, r].start()

    def weight_chunk(src, right, first, count, chunk):
        cols = pl.ds(pl.multiple_of(chunk * per * ds, per * ds), per * ds)
        t = dot_tn(src[:, cols], right[...]).astype(BF16)
        for j in range(per):
            for n in range(count):
                gb[first + n, chunk * per + j] = t[j * ds:(j + 1) * ds, n * cl:(n + 1) * cl]

    def weight_peer_part(src, right, first, count, started):
        if per == 1:
            for o in range(nz):
                for r in range(1, ny):
                    weight_chunk(src, right, first, count, plane(o) * ny + wrap(y + r, ny))
                started(o)
        else:
            for chunk in range(nsp // per):
                weight_chunk(src, right, first, count, chunk)
            for o in range(nz):
                started(o)

    def weight_own_part(src, right, first, count):
        if per == 1:
            for o in range(nz):
                weight_chunk(src, right, first, count, plane(o) * ny + y)

    def out_started(o):
        if o == 0:
            y_start(2, 0)

    weight_peer_part(go, act, 2, 1, out_started)

    for c in st_copies:
        c.wait()
    tsum, tcross = st2[0], st2[1]
    for o in range(ntp - 1):
        tsum = tsum + st2r[o, 0]
        tcross = tcross + st2r[o, 1]
    tsum = tsum / chan * inverse
    tcross = tcross / chan * inverse

    spread(tsum, spa)
    spread(tcross, spb)

    def slope_block(b, c):
        r = pl.ds(pl.multiple_of(b * ROW_BLOCK, ROW_BLOCK), ROW_BLOCK)
        ss = spa[r, :]
        cs = spb[r, :]
        for g in range(groups):
            fut[g, r, :] = nsl[g, r, :] - ss - nrm[g, r, :] * cs
        return c

    slope_block(0, 0)

    @pl.when(has_prev)
    def _():
        back.start()

    for o in range(1, nz):
        y_start(2, o)

    lax.fori_loop(1, nb, slope_block, 0)

    def adjoint_block(b, c):
        r = pl.ds(pl.multiple_of(b * ROW_BLOCK, ROW_BLOCK), ROW_BLOCK)
        for g in range(groups):
            acc = jnp.zeros((ROW_BLOCK, LANES), F32)
            for k in range(tap_count):
                acc = acc + tap(k, g) * fut[g, pl.ds(b * ROW_BLOCK + k, ROW_BLOCK), :]
            s = sg[g, r, :]
            t = acc * s
            sl[r, g * LANES:(g + 1) * LANES] = t.astype(BF16)
            sl[r, cl + g * LANES:cl + (g + 1) * LANES] = (t * val[g, r, :] * (1.0 - s)).astype(BF16)
        return c

    def input_part(i, xx):
        r = slice(i * MATMUL_ROWS, (i + 1) * MATMUL_ROWS)
        blk = pl.ds(pl.multiple_of((2 * xx + core) * dt, dt), dt)
        t = dot_nt(sl[r, 0:cl], wv[blk, :]) + dot_nt(sl[r, cl:2 * cl], wg[blk, :])
        return t + dot_nt(psl[r, 0:cl], pw[xx, 0]) + dot_nt(psl[r, cl:2 * cl], pw[xx, 1])

    xc = []

    def input_send(i):
        slc[i].wait()
        for o in range(1, nx):
            xx = wrap(x + o, nx)
            xs[o - 1, i] = input_part(i, xx).astype(BF16)
            c = remote(xs.at[o - 1, i], xr.at[o - 1, i], x_send.at[o - 1, i], x_recv.at[o - 1, i],
                       {"tp": 2 * xx + core})
            c.start()
            xc.append(c)

    for c in pws:
        c.wait()
    bpc = MATMUL_ROWS // ROW_BLOCK
    slc = []
    for i in range(nrc):
        if i == nrc - 1:
            lax.fori_loop(i * bpc, nb - 1, adjoint_block, 0)

            @pl.when(has_next)
            def _():
                back.wait_recv()

            adjoint_block(nb - 1, 0)
        else:
            lax.fori_loop(i * bpc, (i + 1) * bpc, adjoint_block, 0)
        s = pl.ds(i * MATMUL_ROWS, MATMUL_ROWS)
        c = remote(sl.at[s], psl.at[s], sl_send.at[i], sl_recv.at[i], partner)
        c.start()
        slc.append(c)
        if i > 0:
            input_send(i - 1)

    def vg_started(o):
        if o == nz - 1 or (o == nz - 2 and nh > 1):
            if o == nz - 2:
                y_start(0, o)
                y_start(1, o)
        elif o % 2 == 1:
            for which in range(2):
                y_start(which, o - 1)
                y_start(which, o)

    weight_peer_part(bi, sl, 0, 2, vg_started)
    input_send(nrc - 1)

    weight_own_part(go, act, 2, 1)

    def y_sum(which, u):
        t = gb[which, plane(u) * ny + y].astype(F32)
        for r in range(1, ny):
            y_copies[which, u, r].wait()
            t = t + yb[which, r - 1, u].astype(F32)
        return t

    pair = {"sp": (2 * zh + 1 - zl) * ny + y}
    across = {}

    def a_step(which, h):
        ab[which, h] = y_sum(which, 2 * h).astype(BF16)
        c = remote(ab.at[which, h], ar.at[which, h], a_send.at[which, h], a_recv.at[which, h], pair)
        c.start()
        across[which, h] = c

    def b_sum(which, h):
        t = y_sum(which, 2 * h + 1)
        across[which, h].wait()
        return t + ar[which, h].astype(F32)

    b_copies = {}

    def b_step(which, h):
        bb[which, h] = b_sum(which, h).astype(BF16)
        c = remote(bb.at[which, h], br.at[which, h], b_send.at[which, h], b_recv.at[which, h],
                   {"sp": (2 * wrap(zh + h + 1, nh) + zl) * ny + y})
        c.start()
        b_copies[which, h] = c

    def final_sum(which):
        t = b_sum(which, nh - 1)
        for h in range(nh - 1):
            b_copies[which, h].wait()
            t = t + br[which, h].astype(F32)
        wgrad_ref[which] = t

    for h in range(nh):
        a_step(2, h)

    step = 4
    for g in range(groups):
        def tap_block(b, accs, g=g):
            r = b * 8 * step
            f = fut[g, pl.ds(pl.multiple_of(r, 8 * step), 8 * step), :]
            out = []
            for k in range(tap_count):
                p = f * hist[g, pl.ds(r + (PAD - k), 8 * step), :]
                t = accs[k]
                for i in range(step):
                    t = t + p[8 * i:8 * i + 8]
                out.append(t)
            return tuple(out)

        accs = lax.fori_loop(0, rows // (8 * step), tap_block, (zero,) * tap_count)
        for k in range(tap_count):
            tg[k:k + 1, g * LANES:(g + 1) * LANES] = jnp.sum(accs[k], axis=0, keepdims=True)
        tg[tap_count:tap_count + 1, g * LANES:(g + 1) * LANES] = jnp.sum(gacc[g], axis=0, keepdims=True)

    tzc = []
    for o in range(1, nz):
        c = remote(tg, tgzr.at[o - 1], tz_send.at[o - 1], tz_recv.at[o - 1], {"sp": wrap(z + o, nz) * ny + y})
        c.start()
        tzc.append(c)

    weight_own_part(bi, sl, 0, 2)

    for h in range(nh - 1):
        b_step(2, h)

    def first_part(which, h):
        a_step(which, h)
        if h < nh - 1:
            b_step(which, h)

    if nh > 1:
        a_step(0, 0)
    t = tg[...]
    for o in range(1, nz):
        tzc[o - 1].wait()
        t = t + tgzr[o - 1]
    tgz[...] = t
    tyc = []
    for r in range(1, ny):
        c = remote(tgz, tgy.at[r - 1], ty_send.at[r - 1], ty_recv.at[r - 1], {"sp": z * ny + wrap(y + r, ny)})
        c.start()
        tyc.append(c)
    for o in range(nz - 1 if nh > 1 else nz - 2, nz):
        y_start(0, o)
        y_start(1, o)
    for h in range(nh - 1):
        if h > 0:
            a_step(0, h)
        b_step(0, h)
        a_step(1, h)
        b_step(1, h)

    def input_own(i):
        t = input_part(i, x)
        for o in range(1, nx):
            xc[i * (nx - 1) + o - 1].wait()
            t = t + xr[o - 1, i].astype(F32)
        ig_ref[i * MATMUL_ROWS:(i + 1) * MATMUL_ROWS, :] = t.astype(BF16)

    a_step(0, nh - 1)
    a_step(1, nh - 1)
    final_sum(2)
    for i in range(nrc):
        input_own(i)
    t = tgz[...]
    for r in range(1, ny):
        tyc[r - 1].wait()
        t = t + tgy[r - 1]
    tgrad_ref[...] = t[0:tap_count]
    gaingrad_ref[...] = t[tap_count:tap_count + 1]
    final_sum(0)
    final_sum(1)

    @pl.when(has_next)
    def _():
        halo.wait_send()

    @pl.when(has_prev)
    def _():
        back.wait_send()


def hand_out(ig, wgrad, taps, gain, ig_ref, vgrad_ref, ggrad_ref, ograd_ref, tgrad_ref, gaingrad_ref, out_sem):
    moves = [(wgrad.at[i], ref) for i, ref in enumerate((vgrad_ref, ggrad_ref, ograd_ref))]
    moves += [(ig, ig_ref), (taps, tgrad_ref), (gain, gaingrad_ref)]
    copies = [pltpu.make_async_copy(src, dst, out_sem.at[i]) for i, (src, dst) in enumerate(moves)]
    for c in copies:
        c.start()
    for c in copies:
        c.wait()


def shards(nsp, ntp, block_input, value_proj, gate_proj, conv_taps, norm_gain, out_proj, grad_output):
    rows, width = block_input.shape
    cl = value_proj.shape[1]
    chan = cl * ntp
    nx = ntp // 2
    ny = nx
    nz = nsp // ny
    nh = nz // 2
    nb_slots = max(nh - 1, 1)
    groups = cl // LANES
    ds = width // nsp
    dt = width // ntp
    nrc = rows // MATMUL_ROWS
    tap_count = conv_taps.shape[0]
    dma = pltpu.SemaphoreType.DMA
    vm = pltpu.VMEM
    wide = vm((groups, rows, LANES), F32)
    padded = vm((groups, rows + PAD, LANES), F32)
    tpad = -(-(tap_count + 1) // 8) * 8
    any_spec = pl.BlockSpec(memory_space=pltpu.HBM)
    vmem_spec = pl.BlockSpec(memory_space=pltpu.VMEM)
    outs = pl.pallas_call(
        functools.partial(kernel, (nsp, ntp, ny, nz, nx, float(chan))),
        out_shape=(
            jax.ShapeDtypeStruct((rows, dt), BF16),
            jax.ShapeDtypeStruct((3, ds, cl), F32),
            jax.ShapeDtypeStruct((tap_count, cl), F32),
            jax.ShapeDtypeStruct((1, cl), F32),
        ),
        in_specs=[any_spec] * 7,
        out_specs=[vmem_spec] * 4,
        scratch_shapes=[
            vm((rows, width), BF16), vm((width, cl), BF16), vm((width, cl), BF16), vm((width, cl), BF16),
            vm((rows, width), BF16),
            vm((tap_count, cl), F32), vm((1, cl), F32),
            wide, wide, wide, padded, wide, wide, padded,
            vm((rows, cl), BF16), vm((rows, 2 * cl), BF16), vm((rows, 2 * cl), BF16),
            vm((nx, 2, dt, cl), BF16),
            vm((2, 8, LANES), F32), vm((ntp - 1, 2, 8, LANES), F32),
            vm((2, 8, LANES), F32), vm((ntp - 1, 2, 8, LANES), F32),
            vm((rows, LANES), F32), vm((rows, LANES), F32),
            vm((3, nsp, ds, cl), BF16), vm((3, ny - 1, nz, ds, cl), BF16),
            vm((3, nh, ds, cl), BF16), vm((3, nh, ds, cl), BF16),
            vm((3, nb_slots, ds, cl), BF16), vm((3, nb_slots, ds, cl), BF16),
            vm((nx - 1, nrc, MATMUL_ROWS, dt), BF16), vm((nx - 1, nrc, MATMUL_ROWS, dt), BF16),
            vm((tpad, cl), F32), vm((ny - 1, tpad, cl), F32),
            vm((tpad, cl), F32), vm((nz - 1, tpad, cl), F32),
            dma((6 + nrc,)), dma((4,)),
            dma((2, ntp - 1)), dma((2, ntp - 1)),
            dma((nx, 2)), dma((nx, 2)),
            dma((nrc,)), dma((nrc,)),
            dma((nx - 1, nrc)), dma((nx - 1, nrc)),
            dma((3, ny - 1, nz)), dma((3, ny - 1, nz)),
            dma((3, nh)), dma((3, nh)),
            dma((3, nb_slots)), dma((3, nb_slots)),
            dma((ny - 1,)), dma((ny - 1,)),
            dma((nz - 1,)), dma((nz - 1,)),
        ],
        compiler_params=pltpu.CompilerParams(
            collective_id=0, has_side_effects=True, vmem_limit_bytes=46 * 1000 * 1000),
    )(*[pltpu.with_memory_space_constraint(a, pltpu.HBM) for a in (
        block_input, value_proj, gate_proj, conv_taps, norm_gain.reshape(1, cl), out_proj, grad_output)])
    outs = pl.pallas_call(
        hand_out,
        out_shape=(
            jax.ShapeDtypeStruct((rows, dt), BF16),
            jax.ShapeDtypeStruct((ds, cl), F32),
            jax.ShapeDtypeStruct((ds, cl), F32),
            jax.ShapeDtypeStruct((ds, cl), F32),
            jax.ShapeDtypeStruct((tap_count, cl), F32),
            jax.ShapeDtypeStruct((1, cl), F32),
        ),
        in_specs=[vmem_spec] * 4,
        out_specs=[any_spec] * 6,
        scratch_shapes=[dma((6,))],
        compiler_params=pltpu.CompilerParams(vmem_limit_bytes=8 * 1000 * 1000),
    )(*outs)
    return outs[:5] + (outs[5].reshape(cl),)


def solution(mesh):
    return jax.shard_map(
        functools.partial(shards, mesh.shape["sp"], mesh.shape["tp"]),
        mesh=mesh,
        in_specs=(
            P("sp", None),
            P(None, "tp"),
            P(None, "tp"),
            P(None, "tp"),
            P("tp"),
            P(None, "tp"),
            P("sp", None),
        ),
        out_specs=(
            P("sp", "tp"),
            P("sp", "tp"),
            P("sp", "tp"),
            P("sp", "tp"),
            P(None, "tp"),
            P("tp"),
        ),
        check_vma=False,
    )
```

```python
import functools

import jax
import jax.numpy as jnp
from jax import lax
from jax.experimental import pallas as pl
from jax.experimental.pallas import tpu as pltpu
from jax.sharding import PartitionSpec as P

NORM_FLOOR = 0.1
LANES = 128
ROW_BLOCK = 128
MATMUL_ROWS = 256
PAD = 32
F32 = jnp.float32
BF16 = jnp.bfloat16
MESH = pl.DeviceIdType.MESH


def dot_nt(a, b):
    return lax.dot_general(a, b, (((1,), (1,)), ((), ())), preferred_element_type=F32)


def dot_tn(a, b):
    return lax.dot_general(a, b, (((0,), (0,)), ((), ())), preferred_element_type=F32)


def kernel(cfg, bi_hbm, wv_hbm, wg_hbm, taps_hbm, gain_hbm, wo_hbm, go_hbm,
           ig_ref, wgrad_ref, tgrad_ref, gaingrad_ref,
           bi, wv, wg, wo, go, taps_ref, gain_ref, val, sg, slope, hist, nrm, nsl, fut, act, sl, psl, pw,
           st1, st1r, st2, st2r, spa, spb, gb, yb, zb, zin,
           xs, xr, tg, tgy, tgz, tgzr,
           ld_sem, halo_sem, st_send, st_recv, pw_send, pw_recv, sl_send, sl_recv,
           x_send, x_recv, y_send, y_recv, z_send, z_recv, ty_send, ty_recv, tz_send, tz_recv):
    nsp, ntp, ny, nz, nx, chan = cfg
    rows, width = bi.shape
    cl = wv.shape[1]
    groups = cl // LANES
    tap_count = taps_ref.shape[0]
    nb = rows // ROW_BLOCK
    vpb = ROW_BLOCK // 8
    nrc = rows // MATMUL_ROWS
    ds = width // nsp
    dt = width // ntp
    sp = lax.axis_index("sp")
    tp = lax.axis_index("tp")
    z = sp // ny
    y = sp % ny
    x = tp // 2
    core = tp % 2

    def wrap(v, n):
        return lax.rem(v, n)

    loads = {}

    def load(name, src, dst, i):
        c = pltpu.make_async_copy(src, dst, ld_sem.at[i])
        c.start()
        loads[name] = c

    load("wv", wv_hbm, wv, 0)
    load("wg", wg_hbm, wg, 1)
    for n, i in enumerate(reversed(range(nrc))):
        s = pl.ds(i * MATMUL_ROWS, MATMUL_ROWS)
        load("bi%d" % i, bi_hbm.at[s], bi.at[s], 2 + n)
    load("taps", taps_hbm, taps_ref, 2 + nrc)
    load("gain", gain_hbm, gain_ref, 3 + nrc)
    load("wo", wo_hbm, wo, 4 + nrc)
    load("go", go_hbm, go, 5 + nrc)

    barrier = pltpu.get_barrier_semaphore()
    for o in range(1, nsp):
        pl.semaphore_signal(barrier, inc=1, device_id={"sp": wrap(sp + o, nsp)}, device_id_type=MESH)
    for o in range(1, ntp):
        pl.semaphore_signal(barrier, inc=1, device_id={"tp": wrap(tp + o, ntp)}, device_id_type=MESH)

    def remote(src, dst, ssem, rsem, dev):
        return pltpu.make_async_remote_copy(
            src_ref=src, dst_ref=dst, send_sem=ssem, recv_sem=rsem, device_id=dev, device_id_type=MESH)

    def glu(i):
        r = i * MATMUL_ROWS
        a = bi[r:r + MATMUL_ROWS, :]
        v = jnp.dot(a, wv[...], preferred_element_type=F32)
        s = jax.nn.sigmoid(jnp.dot(a, wg[...], preferred_element_type=F32))
        m = (v * s).astype(BF16).astype(F32)
        for g in range(groups):
            c = slice(g * LANES, (g + 1) * LANES)
            val[g, r:r + MATMUL_ROWS, :] = v[:, c]
            sg[g, r:r + MATMUL_ROWS, :] = s[:, c]
            hist[g, PAD + r:PAD + r + MATMUL_ROWS, :] = m[:, c]

    halo = remote(hist.at[:, pl.ds(rows, PAD), :], hist.at[:, pl.ds(0, PAD), :],
                  halo_sem.at[0], halo_sem.at[1], {"sp": jnp.minimum(sp + 1, nsp - 1)})
    back = remote(fut.at[:, pl.ds(0, PAD), :], fut.at[:, pl.ds(rows, PAD), :],
                  halo_sem.at[2], halo_sem.at[3], {"sp": jnp.maximum(sp - 1, 0)})
    has_next = sp < nsp - 1
    has_prev = sp > 0

    @pl.when(jnp.logical_not(has_prev))
    def _():
        hist[:, 0:PAD, :] = jnp.zeros((groups, PAD, LANES), F32)

    @pl.when(jnp.logical_not(has_next))
    def _():
        fut[:, rows:rows + PAD, :] = jnp.zeros((groups, PAD, LANES), F32)

    lane = lax.broadcasted_iota(jnp.int32, (8, LANES), 1)

    def pack(packed, red, b):
        for i in range(vpb):
            packed = jnp.where(lane == b * vpb + i, red[8 * i:8 * i + 8], packed)
        return packed

    ahead = (lax.broadcasted_iota(jnp.int32, (ROW_BLOCK, LANES), 1)
             - lax.broadcasted_iota(jnp.int32, (ROW_BLOCK, LANES), 0) // 8)
    ones = jnp.ones((3 * LANES, LANES), BF16)

    def spread(packed, dst):
        high = packed.astype(BF16).astype(F32)
        rest = packed - high
        mid = rest.astype(BF16).astype(F32)
        parts = [jnp.concatenate([p] * vpb, axis=0) for p in (high, mid, rest - mid)]
        for b in range(nb):
            own = ahead == b * vpb
            t = jnp.concatenate([jnp.where(own, p, 0.0).astype(BF16) for p in parts], axis=1)
            dst[b * ROW_BLOCK:(b + 1) * ROW_BLOCK, :] = jnp.dot(t, ones, preferred_element_type=F32)

    def tap(k, g):
        return taps_ref[k:k + 1, g * LANES:(g + 1) * LANES]

    def conv_block(b, carry):
        psum, psq = carry
        s = q = None
        for g in range(groups):
            acc = jnp.zeros((ROW_BLOCK, LANES), F32)
            for k in range(tap_count):
                acc = acc + tap(k, g) * hist[g, pl.ds(b * ROW_BLOCK + (PAD - k), ROW_BLOCK), :]
            nrm[g, pl.ds(pl.multiple_of(b * ROW_BLOCK, ROW_BLOCK), ROW_BLOCK), :] = acc
            s = acc if s is None else s + acc
            q = acc * acc if q is None else q + acc * acc
        return (pack(psum, jnp.sum(s, axis=1, keepdims=True), b),
                pack(psq, jnp.sum(q, axis=1, keepdims=True), b))

    zero = jnp.zeros((8, LANES), F32)
    loads["wv"].wait()
    loads["wg"].wait()
    partner = {"tp": 2 * x + 1 - core}
    pws = []
    bpc = MATMUL_ROWS // ROW_BLOCK
    carry = (zero, zero)
    for n, i in enumerate(reversed(range(nrc))):
        if n == 0:
            loads["bi%d" % i].wait()
        else:
            for b in reversed(range(max(i * bpc + bpc + 1, 0), min(i * bpc + 2 * bpc + 1, nb))):
                carry = conv_block(b, carry)
        glu(i)
        if n == 0:
            loads["taps"].wait()
            loads["gain"].wait()
            for j in reversed(range(nrc - 1)):
                loads["bi%d" % j].wait()
            pl.semaphore_wait(barrier, nsp + ntp - 2)

            @pl.when(has_next)
            def _():
                halo.start()

            for xx in range(nx):
                for j, w in enumerate((wv, wg)):
                    first = pl.multiple_of((2 * xx + 1 - core) * dt, dt)
                    c = remote(w.at[pl.ds(first, dt), :], pw.at[xx, j], pw_send.at[xx, j], pw_recv.at[xx, j], partner)
                    c.start()
                    pws.append(c)

    for b in reversed(range(1, bpc + 1)):
        carry = conv_block(b, carry)

    @pl.when(has_prev)
    def _():
        halo.wait_recv()

    psum, psq = conv_block(0, carry)
    st1[0] = psum
    st1[1] = psq

    def share(which, src, dst):
        out = []
        for o in range(1, ntp):
            c = remote(src, dst.at[o - 1], st_send.at[which, o - 1], st_recv.at[which, o - 1],
                       {"tp": wrap(tp + o, ntp)})
            c.start()
            out.append(c)
        return out

    st_copies = share(0, st1, st1r)

    loads["wo"].wait()
    loads["go"].wait()
    for i in range(nrc):
        r = i * MATMUL_ROWS
        t = jnp.dot(go[r:r + MATMUL_ROWS, :], wo[...], preferred_element_type=F32)
        for g in range(groups):
            slope[g, r:r + MATMUL_ROWS, :] = t[:, g * LANES:(g + 1) * LANES]

    for c in st_copies:
        c.wait()
    tsum, tsq = st1[0], st1[1]
    for o in range(ntp - 1):
        tsum = tsum + st1r[o, 0]
        tsq = tsq + st1r[o, 1]
    center = tsum / chan
    inverse = lax.rsqrt(tsq / chan - center * center + NORM_FLOOR)

    spread(center, spa)
    spread(inverse, spb)

    def norm_block(b, carry):
        psum, pcross, gacc = carry
        r = pl.ds(pl.multiple_of(b * ROW_BLOCK, ROW_BLOCK), ROW_BLOCK)
        cen = spa[r, :]
        inv = spb[r, :]
        s = q = None
        gout_acc = []
        for g in range(groups):
            gain = gain_ref[:, g * LANES:(g + 1) * LANES]
            normed = (nrm[g, r, :] - cen) * inv
            scaled = normed * gain
            squash = jax.nn.sigmoid(scaled)
            act[r, g * LANES:(g + 1) * LANES] = (scaled * squash).astype(BF16)
            pre = slope[g, r, :] * squash * (1.0 + scaled * (1.0 - squash))
            pn = pre * normed
            tot = gacc[g]
            for i in range(vpb):
                tot = tot + pn[8 * i:8 * i + 8]
            gout_acc.append(tot)
            ns = pre * gain
            nrm[g, r, :] = normed
            nsl[g, r, :] = ns * inv
            cross = ns * normed
            s = ns if s is None else s + ns
            q = cross if q is None else q + cross
        return (pack(psum, jnp.sum(s, axis=1, keepdims=True), b),
                pack(pcross, jnp.sum(q, axis=1, keepdims=True), b), tuple(gout_acc))

    psum, pcross, gacc = lax.fori_loop(0, nb, norm_block, (zero, zero, (zero,) * groups))
    st2[0] = psum
    st2[1] = pcross
    st_copies = share(1, st2, st2r)

    per = max(1, min(256, width) // ds)
    low = z < nz // 2
    reach = jnp.where(low, nz - 1 - z, z)

    def plane(u):
        if u == nz - 1:
            return z
        up = jnp.where(low, nz - 1 - u, u)
        down = jnp.where(low, u - reach, nz - 1 - (u - reach))
        return jnp.where(u < reach, up, down)

    peers = [(u, r) for u in range(nz) for r in range(1, ny)]

    y_copies = {}
    for which in range(3):
        for o, r in peers:
            yy = wrap(y + r, ny)
            y_copies[which, o, r] = remote(gb.at[which, plane(o) * ny + yy], yb.at[which, r - 1, o],
                                           y_send.at[which, r - 1, o], y_recv.at[which, r - 1, o],
                                           {"sp": z * ny + yy})

    def y_start(which, o):
        for r in range(1, ny):
            y_copies[which, o, r].start()

    def weight_chunk(src, right, first, count, chunk):
        cols = pl.ds(pl.multiple_of(chunk * per * ds, per * ds), per * ds)
        t = dot_tn(src[:, cols], right[...]).astype(BF16)
        for j in range(per):
            for n in range(count):
                gb[first + n, chunk * per + j] = t[j * ds:(j + 1) * ds, n * cl:(n + 1) * cl]

    def weight_peer_part(src, right, first, count, started):
        if per == 1:
            for o in range(nz):
                for r in range(1, ny):
                    weight_chunk(src, right, first, count, plane(o) * ny + wrap(y + r, ny))
                started(o)
        else:
            for chunk in range(nsp // per):
                weight_chunk(src, right, first, count, chunk)
            for o in range(nz):
                started(o)

    def weight_own_part(src, right, first, count, planes):
        if per == 1:
            for o in planes:
                weight_chunk(src, right, first, count, plane(o) * ny + y)

    def y_sum(which, u):
        t = gb[which, plane(u) * ny + y].astype(F32)
        for r in range(1, ny):
            y_copies[which, u, r].wait()
            t = t + yb[which, r - 1, u].astype(F32)
        return t

    def chain_in(which, slot):
        return remote(zin.at[which, slot], zin.at[which, slot], z_send.at[which, 0], z_recv.at[which, slot],
                      {"sp": wrap(z + 1, nz) * ny + y})

    edge = jnp.logical_or(z == 0, z == nz - 1)

    def chain_copy(which, u):
        p = plane(u)
        right = p > z
        slot = jnp.where(p == z - 1, nz, p)
        return remote(zb.at[which, u], zin.at[which, slot], z_send.at[which, u], z_recv.at[which, slot],
                      {"sp": jnp.where(right, z + 1, z - 1) * ny + y})

    def edge_step(which, u):
        @pl.when(edge)
        def _():
            zb[which, u] = y_sum(which, u).astype(BF16)
            chain_copy(which, u).start()

    def middle_step(which, u):
        @pl.when(jnp.logical_not(edge))
        def _():
            t = y_sum(which, u)
            chain_in(which, plane(u)).wait_recv()
            zb[which, u] = (t + zin[which, plane(u)].astype(F32)).astype(BF16)
            chain_copy(which, u).start()

    def final_sum(which):
        wgrad_ref[which] = y_sum(which, nz - 1)

        @pl.when(z > 0)
        def _():
            chain_in(which, z).wait_recv()
            wgrad_ref[which] = wgrad_ref[which] + zin[which, z].astype(F32)

        @pl.when(z < nz - 1)
        def _():
            chain_in(which, nz).wait_recv()
            wgrad_ref[which] = wgrad_ref[which] + zin[which, nz].astype(F32)

    def out_started(o):
        if o == 0:
            y_start(2, 0)

    weight_peer_part(go, act, 2, 1, out_started)
    weight_own_part(go, act, 2, 1, (0,))

    for c in st_copies:
        c.wait()
    tsum, tcross = st2[0], st2[1]
    for o in range(ntp - 1):
        tsum = tsum + st2r[o, 0]
        tcross = tcross + st2r[o, 1]
    tsum = tsum / chan * inverse
    tcross = tcross / chan * inverse

    spread(tsum, spa)
    spread(tcross, spb)

    def slope_block(b, c):
        r = pl.ds(pl.multiple_of(b * ROW_BLOCK, ROW_BLOCK), ROW_BLOCK)
        ss = spa[r, :]
        cs = spb[r, :]
        for g in range(groups):
            fut[g, r, :] = nsl[g, r, :] - ss - nrm[g, r, :] * cs
        return c

    slope_block(0, 0)

    @pl.when(has_prev)
    def _():
        back.start()

    for o in range(1, nz):
        y_start(2, o)

    lax.fori_loop(1, nb, slope_block, 0)

    def adjoint_block(b, c):
        r = pl.ds(pl.multiple_of(b * ROW_BLOCK, ROW_BLOCK), ROW_BLOCK)
        for g in range(groups):
            acc = jnp.zeros((ROW_BLOCK, LANES), F32)
            for k in range(tap_count):
                acc = acc + tap(k, g) * fut[g, pl.ds(b * ROW_BLOCK + k, ROW_BLOCK), :]
            s = sg[g, r, :]
            t = acc * s
            sl[r, g * LANES:(g + 1) * LANES] = t.astype(BF16)
            sl[r, cl + g * LANES:cl + (g + 1) * LANES] = (t * val[g, r, :] * (1.0 - s)).astype(BF16)
        return c

    def input_part(i, xx):
        r = slice(i * MATMUL_ROWS, (i + 1) * MATMUL_ROWS)
        blk = pl.ds(pl.multiple_of((2 * xx + core) * dt, dt), dt)
        t = dot_nt(sl[r, 0:cl], wv[blk, :]) + dot_nt(sl[r, cl:2 * cl], wg[blk, :])
        return t + dot_nt(psl[r, 0:cl], pw[xx, 0]) + dot_nt(psl[r, cl:2 * cl], pw[xx, 1])

    xc = []

    def input_send(i):
        slc[i].wait()
        for o in range(1, nx):
            xx = wrap(x + o, nx)
            xs[o - 1, i] = input_part(i, xx).astype(BF16)
            c = remote(xs.at[o - 1, i], xr.at[o - 1, i], x_send.at[o - 1, i], x_recv.at[o - 1, i],
                       {"tp": 2 * xx + core})
            c.start()
            xc.append(c)

    for c in pws:
        c.wait()
    slc = []
    for i in range(nrc):
        if i == nrc - 1:
            lax.fori_loop(i * bpc, nb - 1, adjoint_block, 0)

            @pl.when(has_next)
            def _():
                back.wait_recv()

            adjoint_block(nb - 1, 0)
        else:
            lax.fori_loop(i * bpc, (i + 1) * bpc, adjoint_block, 0)
        s = pl.ds(i * MATMUL_ROWS, MATMUL_ROWS)
        c = remote(sl.at[s], psl.at[s], sl_send.at[i], sl_recv.at[i], partner)
        c.start()
        slc.append(c)
        if i > 0:
            input_send(i - 1)
        if i == 1:
            edge_step(2, 0)
        if i == 2:
            weight_own_part(go, act, 2, 1, range(1, nz - 2))

    def vg_started(o):
        if o == nz - 2:
            y_start(0, o)
            y_start(1, o)
        elif o < nz - 2 and (o % 2 == 1 or o == nz - 3):
            for which in range(2):
                for v in range(o - o % 2, o + 1):
                    y_start(which, v)

    for u in range(1, nz - 2):
        edge_step(2, u)
    weight_peer_part(bi, sl, 0, 2, vg_started)
    input_send(nrc - 1)
    weight_own_part(go, act, 2, 1, (nz - 2,))
    edge_step(2, nz - 2)
    middle_step(2, 0)
    step = 4
    for g in range(groups):
        def tap_block(b, accs, g=g):
            r = b * 8 * step
            f = fut[g, pl.ds(pl.multiple_of(r, 8 * step), 8 * step), :]
            out = []
            for k in range(tap_count):
                p = f * hist[g, pl.ds(r + (PAD - k), 8 * step), :]
                t = accs[k]
                for i in range(step):
                    t = t + p[8 * i:8 * i + 8]
                out.append(t)
            return tuple(out)

        accs = lax.fori_loop(0, rows // (8 * step), tap_block, (zero,) * tap_count)
        for k in range(tap_count):
            tg[k:k + 1, g * LANES:(g + 1) * LANES] = jnp.sum(accs[k], axis=0, keepdims=True)
        tg[tap_count:tap_count + 1, g * LANES:(g + 1) * LANES] = jnp.sum(gacc[g], axis=0, keepdims=True)

    tzc = []
    for o in range(1, nz):
        c = remote(tg, tgzr.at[o - 1], tz_send.at[o - 1], tz_recv.at[o - 1], {"sp": wrap(z + o, nz) * ny + y})
        c.start()
        tzc.append(c)

    weight_own_part(go, act, 2, 1, (nz - 1,))
    for u in range(1, nz - 2):
        middle_step(2, u)
    weight_own_part(bi, sl, 0, 2, range(nz))
    middle_step(2, nz - 2)

    def input_own(i):
        t = input_part(i, x)
        for o in range(1, nx):
            xc[i * (nx - 1) + o - 1].wait()
            t = t + xr[o - 1, i].astype(F32)
        ig_ref[i * MATMUL_ROWS:(i + 1) * MATMUL_ROWS, :] = t.astype(BF16)

    queue = []
    for u in range(0, nz - 2, 2):
        for which in range(2):
            queue += [(which, v) for v in (u, u + 1) if v < nz - 2]
    queue += [(0, nz - 2), (1, nz - 2)]
    middle = queue[:-3] + [queue[-2], queue[-3], queue[-1]]
    tyc = []
    for n, item in enumerate(queue):
        edge_step(*item)
        if n == 3:
            t = tg[...]
            for o in range(1, nz):
                tzc[o - 1].wait()
                t = t + tgzr[o - 1]
            tgz[...] = t
            for r in range(1, ny):
                c = remote(tgz, tgy.at[r - 1], ty_send.at[r - 1], ty_recv.at[r - 1],
                           {"sp": z * ny + wrap(y + r, ny)})
                c.start()
                tyc.append(c)
            y_start(0, nz - 1)
            y_start(1, nz - 1)
        if n > 0:
            middle_step(*middle[n - 1])
        if n < 2 * nrc and n % 2 == 0:
            input_own(n // 2)
    middle_step(*middle[-1])
    for i in range(min(nrc, (len(queue) + 1) // 2), nrc):
        input_own(i)
    final_sum(2)
    t = tgz[...]
    for r in range(1, ny):
        tyc[r - 1].wait()
        t = t + tgy[r - 1]
    tgrad_ref[...] = t[0:tap_count]
    gaingrad_ref[...] = t[tap_count:tap_count + 1]
    final_sum(0)
    final_sum(1)
    for which in range(3):
        for u in range(nz - 1):
            chain_copy(which, u).wait_send()

    @pl.when(has_next)
    def _():
        halo.wait_send()

    @pl.when(has_prev)
    def _():
        back.wait_send()


def hand_out(ig, wgrad, taps, gain, ig_ref, vgrad_ref, ggrad_ref, ograd_ref, tgrad_ref, gaingrad_ref, out_sem):
    moves = [(wgrad.at[i], ref) for i, ref in enumerate((vgrad_ref, ggrad_ref, ograd_ref))]
    moves += [(ig, ig_ref), (taps, tgrad_ref), (gain, gaingrad_ref)]
    copies = [pltpu.make_async_copy(src, dst, out_sem.at[i]) for i, (src, dst) in enumerate(moves)]
    for c in copies:
        c.start()
    for c in copies:
        c.wait()


def shards(nsp, ntp, block_input, value_proj, gate_proj, conv_taps, norm_gain, out_proj, grad_output):
    rows, width = block_input.shape
    cl = value_proj.shape[1]
    chan = cl * ntp
    nx = ntp // 2
    ny = nx
    nz = nsp // ny
    groups = cl // LANES
    ds = width // nsp
    dt = width // ntp
    nrc = rows // MATMUL_ROWS
    tap_count = conv_taps.shape[0]
    dma = pltpu.SemaphoreType.DMA
    vm = pltpu.VMEM
    wide = vm((groups, rows, LANES), F32)
    padded = vm((groups, rows + PAD, LANES), F32)
    tpad = -(-(tap_count + 1) // 8) * 8
    any_spec = pl.BlockSpec(memory_space=pltpu.HBM)
    vmem_spec = pl.BlockSpec(memory_space=pltpu.VMEM)
    outs = pl.pallas_call(
        functools.partial(kernel, (nsp, ntp, ny, nz, nx, float(chan))),
        out_shape=(
            jax.ShapeDtypeStruct((rows, dt), BF16),
            jax.ShapeDtypeStruct((3, ds, cl), F32),
            jax.ShapeDtypeStruct((tap_count, cl), F32),
            jax.ShapeDtypeStruct((1, cl), F32),
        ),
        in_specs=[any_spec] * 7,
        out_specs=[vmem_spec] * 4,
        scratch_shapes=[
            vm((rows, width), BF16), vm((width, cl), BF16), vm((width, cl), BF16), vm((width, cl), BF16),
            vm((rows, width), BF16),
            vm((tap_count, cl), F32), vm((1, cl), F32),
            wide, wide, wide, padded, wide, wide, padded,
            vm((rows, cl), BF16), vm((rows, 2 * cl), BF16), vm((rows, 2 * cl), BF16),
            vm((nx, 2, dt, cl), BF16),
            vm((2, 8, LANES), F32), vm((ntp - 1, 2, 8, LANES), F32),
            vm((2, 8, LANES), F32), vm((ntp - 1, 2, 8, LANES), F32),
            vm((rows, LANES), F32), vm((rows, LANES), F32),
            vm((3, nsp, ds, cl), BF16), vm((3, ny - 1, nz, ds, cl), BF16),
            vm((3, nz - 1, ds, cl), BF16), vm((3, nz + 1, ds, cl), BF16),
            vm((nx - 1, nrc, MATMUL_ROWS, dt), BF16), vm((nx - 1, nrc, MATMUL_ROWS, dt), BF16),
            vm((tpad, cl), F32), vm((ny - 1, tpad, cl), F32),
            vm((tpad, cl), F32), vm((nz - 1, tpad, cl), F32),
            dma((6 + nrc,)), dma((4,)),
            dma((2, ntp - 1)), dma((2, ntp - 1)),
            dma((nx, 2)), dma((nx, 2)),
            dma((nrc,)), dma((nrc,)),
            dma((nx - 1, nrc)), dma((nx - 1, nrc)),
            dma((3, ny - 1, nz)), dma((3, ny - 1, nz)),
            dma((3, nz - 1)), dma((3, nz + 1)),
            dma((ny - 1,)), dma((ny - 1,)),
            dma((nz - 1,)), dma((nz - 1,)),
        ],
        compiler_params=pltpu.CompilerParams(
            collective_id=0, has_side_effects=True, vmem_limit_bytes=46 * 1000 * 1000),
    )(*[pltpu.with_memory_space_constraint(a, pltpu.HBM) for a in (
        block_input, value_proj, gate_proj, conv_taps, norm_gain.reshape(1, cl), out_proj, grad_output)])
    outs = pl.pallas_call(
        hand_out,
        out_shape=(
            jax.ShapeDtypeStruct((rows, dt), BF16),
            jax.ShapeDtypeStruct((ds, cl), F32),
            jax.ShapeDtypeStruct((ds, cl), F32),
            jax.ShapeDtypeStruct((ds, cl), F32),
            jax.ShapeDtypeStruct((tap_count, cl), F32),
            jax.ShapeDtypeStruct((1, cl), F32),
        ),
        in_specs=[vmem_spec] * 4,
        out_specs=[any_spec] * 6,
        scratch_shapes=[dma((6,))],
        compiler_params=pltpu.CompilerParams(vmem_limit_bytes=8 * 1000 * 1000),
    )(*outs)
    return outs[:5] + (outs[5].reshape(cl),)


def solution(mesh):
    return jax.shard_map(
        functools.partial(shards, mesh.shape["sp"], mesh.shape["tp"]),
        mesh=mesh,
        in_specs=(
            P("sp", None),
            P(None, "tp"),
            P(None, "tp"),
            P(None, "tp"),
            P("tp"),
            P(None, "tp"),
            P("sp", None),
        ),
        out_specs=(
            P("sp", "tp"),
            P("sp", "tp"),
            P("sp", "tp"),
            P("sp", "tp"),
            P(None, "tp"),
            P("tp"),
        ),
        check_vma=False,
    )
```

```python
import functools

import jax
import jax.numpy as jnp
from jax import lax
from jax.experimental import pallas as pl
from jax.experimental.pallas import tpu as pltpu
from jax.sharding import PartitionSpec as P

NORM_FLOOR = 0.1
LANES = 128
ROW_BLOCK = 128
MATMUL_ROWS = 256
PAD = 32
EARLY_FROM = 4
F32 = jnp.float32
BF16 = jnp.bfloat16
MESH = pl.DeviceIdType.MESH


def dot_nt(a, b):
    return lax.dot_general(a, b, (((1,), (1,)), ((), ())), preferred_element_type=F32)


def dot_tn(a, b):
    return lax.dot_general(a, b, (((0,), (0,)), ((), ())), preferred_element_type=F32)


def kernel(cfg, bi_hbm, wv_hbm, wg_hbm, taps_hbm, gain_hbm, wo_hbm, go_hbm,
           ig_ref, wgrad_ref, tgrad_ref, gaingrad_ref,
           bi, wv, wg, wo, go, taps_ref, gain_ref, val, sg, slope, hist, nrm, nsl, fut, act, sl, psl, pw,
           st1, st1r, st2, st2r, spa, spb, gb, yb, zb, zin, eb, ein, ey, ef,
           xs, xr, tg, tgb, tgy, tgz, tgzr,
           ld_sem, halo_sem, st_send, st_recv, pw_send, pw_recv, sl_send, sl_recv,
           x_send, x_recv, y_send, y_recv, z_send, z_recv, e_send, e_recv, ey_send, ey_recv, ty_send, ty_recv, tz_send, tz_recv):
    nsp, ntp, ny, nz, nx, chan = cfg
    rows, width = bi.shape
    cl = wv.shape[1]
    groups = cl // LANES
    tap_count = taps_ref.shape[0]
    nb = rows // ROW_BLOCK
    vpb = ROW_BLOCK // 8
    nrc = rows // MATMUL_ROWS
    ds = width // nsp
    dt = width // ntp
    sp = lax.axis_index("sp")
    tp = lax.axis_index("tp")
    z = sp // ny
    y = sp % ny
    x = tp // 2
    core = tp % 2

    def wrap(v, n):
        return lax.rem(v, n)

    loads = {}

    def load(name, src, dst, i):
        c = pltpu.make_async_copy(src, dst, ld_sem.at[i])
        c.start()
        loads[name] = c

    load("wv", wv_hbm, wv, 0)
    load("wg", wg_hbm, wg, 1)
    for n, i in enumerate(reversed(range(nrc))):
        s = pl.ds(i * MATMUL_ROWS, MATMUL_ROWS)
        load("bi%d" % i, bi_hbm.at[s], bi.at[s], 2 + n)
    load("taps", taps_hbm, taps_ref, 2 + nrc)
    load("gain", gain_hbm, gain_ref, 3 + nrc)
    load("wo", wo_hbm, wo, 4 + nrc)
    load("go", go_hbm, go, 5 + nrc)

    barrier = pltpu.get_barrier_semaphore()
    for o in range(1, nsp):
        pl.semaphore_signal(barrier, inc=1, device_id={"sp": wrap(sp + o, nsp)}, device_id_type=MESH)
    for o in range(1, ntp):
        pl.semaphore_signal(barrier, inc=1, device_id={"tp": wrap(tp + o, ntp)}, device_id_type=MESH)

    def remote(src, dst, ssem, rsem, dev):
        return pltpu.make_async_remote_copy(
            src_ref=src, dst_ref=dst, send_sem=ssem, recv_sem=rsem, device_id=dev, device_id_type=MESH)

    def glu(i):
        r = i * MATMUL_ROWS
        a = bi[r:r + MATMUL_ROWS, :]
        v = jnp.dot(a, wv[...], preferred_element_type=F32)
        s = jax.nn.sigmoid(jnp.dot(a, wg[...], preferred_element_type=F32))
        m = (v * s).astype(BF16).astype(F32)
        for g in range(groups):
            c = slice(g * LANES, (g + 1) * LANES)
            val[g, r:r + MATMUL_ROWS, :] = v[:, c]
            sg[g, r:r + MATMUL_ROWS, :] = s[:, c]
            hist[g, PAD + r:PAD + r + MATMUL_ROWS, :] = m[:, c]

    halo = remote(hist.at[:, pl.ds(rows, PAD), :], hist.at[:, pl.ds(0, PAD), :],
                  halo_sem.at[0], halo_sem.at[1], {"sp": jnp.minimum(sp + 1, nsp - 1)})
    back = remote(fut.at[:, pl.ds(0, PAD), :], fut.at[:, pl.ds(rows, PAD), :],
                  halo_sem.at[2], halo_sem.at[3], {"sp": jnp.maximum(sp - 1, 0)})
    has_next = sp < nsp - 1
    has_prev = sp > 0

    @pl.when(jnp.logical_not(has_prev))
    def _():
        hist[:, 0:PAD, :] = jnp.zeros((groups, PAD, LANES), F32)

    @pl.when(jnp.logical_not(has_next))
    def _():
        fut[:, rows:rows + PAD, :] = jnp.zeros((groups, PAD, LANES), F32)

    lane = lax.broadcasted_iota(jnp.int32, (8, LANES), 1)

    def pack(packed, red, b):
        for i in range(vpb):
            packed = jnp.where(lane == b * vpb + i, red[8 * i:8 * i + 8], packed)
        return packed

    ahead = (lax.broadcasted_iota(jnp.int32, (ROW_BLOCK, LANES), 1)
             - lax.broadcasted_iota(jnp.int32, (ROW_BLOCK, LANES), 0) // 8)
    ones = jnp.ones((3 * LANES, LANES), BF16)

    def spread(packed, dst):
        high = packed.astype(BF16).astype(F32)
        rest = packed - high
        mid = rest.astype(BF16).astype(F32)
        parts = [jnp.concatenate([p] * vpb, axis=0) for p in (high, mid, rest - mid)]
        for b in range(nb):
            own = ahead == b * vpb
            t = jnp.concatenate([jnp.where(own, p, 0.0).astype(BF16) for p in parts], axis=1)
            dst[b * ROW_BLOCK:(b + 1) * ROW_BLOCK, :] = jnp.dot(t, ones, preferred_element_type=F32)

    def tap(k, g):
        return taps_ref[k:k + 1, g * LANES:(g + 1) * LANES]

    def conv_block(b, carry):
        psum, psq = carry
        s = q = None
        for g in range(groups):
            acc = jnp.zeros((ROW_BLOCK, LANES), F32)
            for k in range(tap_count):
                acc = acc + tap(k, g) * hist[g, pl.ds(b * ROW_BLOCK + (PAD - k), ROW_BLOCK), :]
            nrm[g, pl.ds(pl.multiple_of(b * ROW_BLOCK, ROW_BLOCK), ROW_BLOCK), :] = acc
            s = acc if s is None else s + acc
            q = acc * acc if q is None else q + acc * acc
        return (pack(psum, jnp.sum(s, axis=1, keepdims=True), b),
                pack(psq, jnp.sum(q, axis=1, keepdims=True), b))

    zero = jnp.zeros((8, LANES), F32)
    loads["wv"].wait()
    loads["wg"].wait()
    partner = {"tp": 2 * x + 1 - core}
    pws = []
    bpc = MATMUL_ROWS // ROW_BLOCK
    carry = (zero, zero)
    for n, i in enumerate(reversed(range(nrc))):
        if n == 0:
            loads["bi%d" % i].wait()
        else:
            for b in reversed(range(max(i * bpc + bpc + 1, 0), min(i * bpc + 2 * bpc + 1, nb))):
                carry = conv_block(b, carry)
        glu(i)
        if n == 0:
            loads["taps"].wait()
            loads["gain"].wait()
            for j in reversed(range(nrc - 1)):
                loads["bi%d" % j].wait()
            pl.semaphore_wait(barrier, nsp + ntp - 2)

            @pl.when(has_next)
            def _():
                halo.start()

            for xx in range(nx):
                for j, w in enumerate((wv, wg)):
                    first = pl.multiple_of((2 * xx + 1 - core) * dt, dt)
                    c = remote(w.at[pl.ds(first, dt), :], pw.at[xx, j], pw_send.at[xx, j], pw_recv.at[xx, j], partner)
                    c.start()
                    pws.append(c)

    for b in reversed(range(1, bpc + 1)):
        carry = conv_block(b, carry)

    @pl.when(has_prev)
    def _():
        halo.wait_recv()

    psum, psq = conv_block(0, carry)
    st1[0] = psum
    st1[1] = psq

    def share(which, src, dst):
        out = []
        for o in range(1, ntp):
            c = remote(src, dst.at[o - 1], st_send.at[which, o - 1], st_recv.at[which, o - 1],
                       {"tp": wrap(tp + o, ntp)})
            c.start()
            out.append(c)
        return out

    st_copies = share(0, st1, st1r)

    loads["wo"].wait()
    loads["go"].wait()
    for i in range(nrc):
        r = i * MATMUL_ROWS
        t = jnp.dot(go[r:r + MATMUL_ROWS, :], wo[...], preferred_element_type=F32)
        for g in range(groups):
            slope[g, r:r + MATMUL_ROWS, :] = t[:, g * LANES:(g + 1) * LANES]

    for c in st_copies:
        c.wait()
    tsum, tsq = st1[0], st1[1]
    for o in range(ntp - 1):
        tsum = tsum + st1r[o, 0]
        tsq = tsq + st1r[o, 1]
    center = tsum / chan
    inverse = lax.rsqrt(tsq / chan - center * center + NORM_FLOOR)

    spread(center, spa)
    spread(inverse, spb)

    def norm_block(b, carry):
        psum, pcross, gacc = carry
        r = pl.ds(pl.multiple_of(b * ROW_BLOCK, ROW_BLOCK), ROW_BLOCK)
        cen = spa[r, :]
        inv = spb[r, :]
        s = q = None
        gout_acc = []
        for g in range(groups):
            gain = gain_ref[:, g * LANES:(g + 1) * LANES]
            normed = (nrm[g, r, :] - cen) * inv
            scaled = normed * gain
            squash = jax.nn.sigmoid(scaled)
            act[r, g * LANES:(g + 1) * LANES] = (scaled * squash).astype(BF16)
            pre = slope[g, r, :] * squash * (1.0 + scaled * (1.0 - squash))
            pn = pre * normed
            tot = gacc[g]
            for i in range(vpb):
                tot = tot + pn[8 * i:8 * i + 8]
            gout_acc.append(tot)
            ns = pre * gain
            nrm[g, r, :] = normed
            nsl[g, r, :] = ns * inv
            cross = ns * normed
            s = ns if s is None else s + ns
            q = cross if q is None else q + cross
        return (pack(psum, jnp.sum(s, axis=1, keepdims=True), b),
                pack(pcross, jnp.sum(q, axis=1, keepdims=True), b), tuple(gout_acc))

    psum, pcross, gacc = lax.fori_loop(0, nb, norm_block, (zero, zero, (zero,) * groups))
    st2[0] = psum
    st2[1] = pcross
    st_copies = share(1, st2, st2r)

    per = max(1, min(256, width) // ds)
    low = z < nz // 2
    reach = jnp.where(low, nz - 1 - z, z)

    def plane(u):
        if u == nz - 1:
            return z
        up = jnp.where(low, nz - 1 - u, u)
        down = jnp.where(low, u - reach, nz - 1 - (u - reach))
        return jnp.where(u < reach, up, down)

    peers = [(u, r) for u in range(nz) for r in range(1, ny)]

    half = ds * EARLY_FROM // 8
    share_rows = (ds, ds, half)
    y_copies = {}
    for which in range(3):
        for o, r in peers:
            yy = wrap(y + r, ny)
            rs = pl.ds(0, share_rows[which])
            y_copies[which, o, r] = remote(gb.at[which, plane(o) * ny + yy, rs], yb.at[which, r - 1, o, rs],
                                           y_send.at[which, r - 1, o], y_recv.at[which, r - 1, o],
                                           {"sp": z * ny + yy})

    def y_start(which, o):
        for r in range(1, ny):
            y_copies[which, o, r].start()

    def weight_chunk(src, right, first, count, chunk, between=None):
        cols = pl.ds(pl.multiple_of(chunk * per * ds, per * ds), per * ds)
        if between is None:
            t = dot_tn(src[:, cols], right[...])
        else:
            t = None
            for k in range(nrc):
                rs = pl.ds(k * MATMUL_ROWS, MATMUL_ROWS)
                d = dot_tn(src[rs, cols], right[rs, :])
                t = d if t is None else t + d
                between(k)
        t = t.astype(BF16)
        for j in range(per):
            for n in range(count):
                gb[first + n, chunk * per + j] = t[j * ds:(j + 1) * ds, n * cl:(n + 1) * cl]

    def weight_peer(src, right, first, count, o, between=None):
        if per == 1:
            for r in range(1, ny):
                weight_chunk(src, right, first, count, plane(o) * ny + wrap(y + r, ny), between if r == 1 else None)
            between = None
        elif o == 0:
            for chunk in range(nsp // per):
                weight_chunk(src, right, first, count, chunk)
        if between is not None:
            for k in range(nrc):
                between(k)

    def weight_own(src, right, first, count, o, between=None):
        if per == 1:
            weight_chunk(src, right, first, count, plane(o) * ny + y, between)
        elif between is not None:
            for k in range(nrc):
                between(k)

    def y_sum(which, u):
        n = share_rows[which]
        t = gb[which, plane(u) * ny + y, 0:n].astype(F32)
        for r in range(1, ny):
            y_copies[which, u, r].wait()
            t = t + yb[which, r - 1, u, 0:n].astype(F32)
        return t

    def chain_in(which, slot):
        rs = pl.ds(0, share_rows[which])
        return remote(zin.at[which, slot, rs], zin.at[which, slot, rs], z_send.at[which, 0], z_recv.at[which, slot],
                      {"sp": wrap(z + 1, nz) * ny + y})

    edge = jnp.logical_or(z == 0, z == nz - 1)

    def chain_to(u):
        p = plane(u)
        return jnp.where(p == z - 1, nz, p), {"sp": jnp.where(p > z, z + 1, z - 1) * ny + y}

    def chain_copy(which, u):
        slot, dev = chain_to(u)
        rs = pl.ds(0, share_rows[which])
        return remote(zb.at[which, u, rs], zin.at[which, slot, rs], z_send.at[which, u], z_recv.at[which, slot], dev)

    def edge_step(which, u):
        @pl.when(edge)
        def _():
            zb[which, u, 0:share_rows[which]] = y_sum(which, u).astype(BF16)
            chain_copy(which, u).start()

    def middle_step(which, u):
        @pl.when(jnp.logical_not(edge))
        def _():
            n = share_rows[which]
            t = y_sum(which, u)
            chain_in(which, plane(u)).wait_recv()
            zb[which, u, 0:n] = (t + zin[which, plane(u), 0:n].astype(F32)).astype(BF16)
            chain_copy(which, u).start()

    def final_sum(which):
        n = share_rows[which]
        wgrad_ref[which, 0:n] = y_sum(which, nz - 1)

        @pl.when(z > 0)
        def _():
            chain_in(which, z).wait_recv()
            wgrad_ref[which, 0:n] = wgrad_ref[which, 0:n] + zin[which, z, 0:n].astype(F32)

        @pl.when(z < nz - 1)
        def _():
            chain_in(which, nz).wait_recv()
            wgrad_ref[which, 0:n] = wgrad_ref[which, 0:n] + zin[which, nz, 0:n].astype(F32)

    def early_in(slot):
        return remote(ein.at[slot], ein.at[slot], e_send.at[0], e_recv.at[slot], {"sp": wrap(z + 1, nz) * ny + y})

    def early_copy(u, src):
        slot, dev = chain_to(u)
        return remote(src, ein.at[slot], e_send.at[u], e_recv.at[slot], dev)

    def early_own(p):
        return gb[2, pl.ds(p * ny, ny), half:ds].astype(F32)

    def early_edge(u):
        @pl.when(edge)
        def _():
            early_copy(u, gb.at[2, pl.ds(plane(u) * ny, ny), pl.ds(half, ds - half)]).start()

    def early_middle(u):
        @pl.when(jnp.logical_not(edge))
        def _():
            early_in(plane(u)).wait_recv()
            eb[u] = (early_own(plane(u)) + ein[plane(u)].astype(F32)).astype(BF16)
            early_copy(u, eb.at[u]).start()

    early_y = []
    for r in range(1, ny):
        yy = wrap(y + r, ny)
        early_y.append(remote(eb.at[nz - 1, yy], ey.at[r - 1], ey_send.at[r - 1], ey_recv.at[r - 1],
                              {"sp": z * ny + yy}))

    def early_turn():
        ef[...] = early_own(z)

        @pl.when(z > 0)
        def _():
            early_in(z).wait_recv()
            ef[...] = ef[...] + ein[z].astype(F32)

        @pl.when(z < nz - 1)
        def _():
            early_in(nz).wait_recv()
            ef[...] = ef[...] + ein[nz].astype(F32)

        eb[nz - 1] = ef[...].astype(BF16)
        for c in early_y:
            c.start()

    def early_final():
        t = ef[y]
        for r in range(1, ny):
            early_y[r - 1].wait()
            t = t + ey[r - 1].astype(F32)
        wgrad_ref[2, half:ds] = t

    weight_peer(go, act, 2, 1, 0)
    y_start(2, 0)
    weight_own(go, act, 2, 1, 0)
    early_edge(0)
    weight_peer(go, act, 2, 1, 1)
    y_start(2, 1)
    weight_own(go, act, 2, 1, 1)
    for o in range(2, nz - 1):
        weight_peer(go, act, 2, 1, o)

    for c in st_copies:
        c.wait()
    tsum, tcross = st2[0], st2[1]
    for o in range(ntp - 1):
        tsum = tsum + st2r[o, 0]
        tcross = tcross + st2r[o, 1]
    tsum = tsum / chan * inverse
    tcross = tcross / chan * inverse

    spread(tsum, spa)
    spread(tcross, spb)

    def slope_block(b, c):
        r = pl.ds(pl.multiple_of(b * ROW_BLOCK, ROW_BLOCK), ROW_BLOCK)
        ss = spa[r, :]
        cs = spb[r, :]
        for g in range(groups):
            fut[g, r, :] = nsl[g, r, :] - ss - nrm[g, r, :] * cs
        return c

    slope_block(0, 0)

    @pl.when(has_prev)
    def _():
        back.start()

    for o in range(2, nz - 1):
        y_start(2, o)
    early_edge(1)

    lax.fori_loop(1, nb, slope_block, 0)

    def adjoint_block(b, only=None):
        r = pl.ds(pl.multiple_of(b * ROW_BLOCK, ROW_BLOCK), ROW_BLOCK)
        for g in range(groups) if only is None else only:
            acc = jnp.zeros((ROW_BLOCK, LANES), F32)
            for k in range(tap_count):
                acc = acc + tap(k, g) * fut[g, pl.ds(b * ROW_BLOCK + k, ROW_BLOCK), :]
            s = sg[g, r, :]
            t = acc * s
            sl[r, g * LANES:(g + 1) * LANES] = t.astype(BF16)
            sl[r, cl + g * LANES:cl + (g + 1) * LANES] = (t * val[g, r, :] * (1.0 - s)).astype(BF16)

    def input_part(i, xx):
        r = slice(i * MATMUL_ROWS, (i + 1) * MATMUL_ROWS)
        blk = pl.ds(pl.multiple_of((2 * xx + core) * dt, dt), dt)
        t = dot_nt(sl[r, 0:cl], wv[blk, :]) + dot_nt(sl[r, cl:2 * cl], wg[blk, :])
        return t + dot_nt(psl[r, 0:cl], pw[xx, 0]) + dot_nt(psl[r, cl:2 * cl], pw[xx, 1])

    xc = []

    def input_send(i):
        for o in range(1, nx):
            xx = wrap(x + o, nx)
            xs[o - 1, i] = input_part(i, xx).astype(BF16)
            c = remote(xs.at[o - 1, i], xr.at[o - 1, i], x_send.at[o - 1, i], x_recv.at[o - 1, i],
                       {"tp": 2 * xx + core})
            c.start()
            xc.append(c)

    for c in pws:
        c.wait()
    slc = []
    for i in range(nrc):
        if i == 2:
            slc[0].wait()
        todo = [(b, g) for b in range(i * bpc, nb - 1 if i == nrc - 1 else (i + 1) * bpc) for g in range(groups)]

        def between(k, todo=todo):
            for b, g in todo[k * len(todo) // nrc:(k + 1) * len(todo) // nrc]:
                adjoint_block(b, (g,))

        if not (i == 0 or i == 1):
            for k in range(nrc):
                between(k)
        if i == 2:
            input_send(0)
        if i == 0:
            for o in range(2, nz - 1):
                weight_own(go, act, 2, 1, o, between if o == 2 else None)
                early_edge(o)
        if i == 1:
            weight_peer(go, act, 2, 1, nz - 1, between)
            y_start(2, nz - 1)
        if i == nrc - 1:
            early_middle(0)

            @pl.when(has_next)
            def _():
                back.wait_recv()

            adjoint_block(nb - 1)
        s = pl.ds(i * MATMUL_ROWS, MATMUL_ROWS)
        c = remote(sl.at[s], psl.at[s], sl_send.at[i], sl_recv.at[i], partner)
        c.start()
        slc.append(c)

    for o in range(nz):
        weight_peer(bi, sl, 0, 2, o)
        if o == 0:
            y_start(0, 0)
        elif o < nz - 2 and (o % 2 == 1 or o == nz - 3):
            for which in range(2):
                for v in range(o - o % 2, o + 1):
                    if which or v:
                        y_start(which, v)
        elif o == nz - 2:
            y_start(0, o)
            y_start(1, o)

    for u in range(nz - 1):
        edge_step(2, u)
    for i in range(1, nrc - 1):
        slc[i].wait()
        input_send(i)
    early_middle(1)
    weight_own(go, act, 2, 1, nz - 1)
    for o in range(nz):
        weight_own(bi, sl, 0, 2, o)
    edge_step(0, 0)
    slc[nrc - 1].wait()
    input_send(nrc - 1)

    step = 4
    def taps_part(g):
        def tap_block(b, accs):
            r = b * 8 * step
            f = fut[g, pl.ds(pl.multiple_of(r, 8 * step), 8 * step), :]
            out = []
            for k in range(tap_count):
                p = f * hist[g, pl.ds(r + (PAD - k), 8 * step), :]
                t = accs[k]
                for i in range(step):
                    t = t + p[8 * i:8 * i + 8]
                out.append(t)
            return tuple(out)

        accs = lax.fori_loop(0, rows // (8 * step), tap_block, (zero,) * tap_count)
        for k in range(tap_count):
            tg[k:k + 1, g * LANES:(g + 1) * LANES] = jnp.sum(accs[k], axis=0, keepdims=True)
        tg[tap_count:tap_count + 1, g * LANES:(g + 1) * LANES] = jnp.sum(gacc[g], axis=0, keepdims=True)

    def input_own(i):
        t = input_part(i, x)
        for o in range(1, nx):
            xc[i * (nx - 1) + o - 1].wait()
            t = t + xr[o - 1, i].astype(F32)
        ig_ref[i * MATMUL_ROWS:(i + 1) * MATMUL_ROWS, :] = t.astype(BF16)

    queue = []
    for u in range(0, nz - 2, 2):
        for which in range(2):
            queue += [(which, v) for v in (u, u + 1) if v < nz - 2]
    queue += [(0, nz - 2), (1, nz - 2)]
    middle = queue[:-3] + [queue[-2], queue[-3], queue[-1]]

    taps_part(0)
    for u in range(2, nz - 1):
        early_middle(u)
    middle_step(2, 0)
    edge_step(*queue[1])
    for g in range(1, groups):
        taps_part(g)
    tgb[...] = tg[...].astype(BF16)
    tzc = []
    for o in range(1, nz):
        c = remote(tgb, tgzr.at[o - 1], tz_send.at[o - 1], tz_recv.at[o - 1], {"sp": wrap(z + o, nz) * ny + y})
        c.start()
        tzc.append(c)

    for u in range(1, nz - 2):
        middle_step(2, u)
    edge_step(*queue[2])
    middle_step(2, nz - 2)
    middle_step(*middle[0])
    early_turn()
    y_start(0, nz - 1)
    edge_step(*queue[3])
    tyc = []
    done = 0
    for n in range(1, len(queue)):
        middle_step(*middle[n])
        if n == 1:
            input_own(done)
            done += 1
        if n + 3 < len(queue):
            edge_step(*queue[n + 3])
        if n == 2:
            t = tgb[...].astype(F32)
            for o in range(1, nz):
                tzc[o - 1].wait()
                t = t + tgzr[o - 1].astype(F32)
            tgz[...] = t.astype(BF16)
            for r in range(1, ny):
                c = remote(tgz, tgy.at[r - 1], ty_send.at[r - 1], ty_recv.at[r - 1],
                           {"sp": z * ny + wrap(y + r, ny)})
                c.start()
                tyc.append(c)
            y_start(1, nz - 1)
        if n > 2 and done < nrc - 1:
            input_own(done)
            done += 1
    for i in range(done, nrc):
        input_own(i)
    early_final()
    final_sum(2)
    t = tgz[...].astype(F32)
    for r in range(1, ny):
        tyc[r - 1].wait()
        t = t + tgy[r - 1].astype(F32)
    tgrad_ref[...] = t[0:tap_count]
    gaingrad_ref[...] = t[tap_count:tap_count + 1]
    final_sum(0)
    final_sum(1)
    for u in range(nz - 1):
        early_copy(u, eb.at[u]).wait_send()
        for which in range(3):
            chain_copy(which, u).wait_send()

    @pl.when(has_next)
    def _():
        halo.wait_send()

    @pl.when(has_prev)
    def _():
        back.wait_send()


def hand_out(ig, wgrad, taps, gain, ig_ref, vgrad_ref, ggrad_ref, ograd_ref, tgrad_ref, gaingrad_ref, out_sem):
    moves = [(wgrad.at[i], ref) for i, ref in enumerate((vgrad_ref, ggrad_ref, ograd_ref))]
    moves += [(ig, ig_ref), (taps, tgrad_ref), (gain, gaingrad_ref)]
    copies = [pltpu.make_async_copy(src, dst, out_sem.at[i]) for i, (src, dst) in enumerate(moves)]
    for c in copies:
        c.start()
    for c in copies:
        c.wait()


def shards(nsp, ntp, block_input, value_proj, gate_proj, conv_taps, norm_gain, out_proj, grad_output):
    rows, width = block_input.shape
    cl = value_proj.shape[1]
    chan = cl * ntp
    nx = ntp // 2
    ny = nx
    nz = nsp // ny
    groups = cl // LANES
    ds = width // nsp
    late = ds - ds * EARLY_FROM // 8
    dt = width // ntp
    nrc = rows // MATMUL_ROWS
    tap_count = conv_taps.shape[0]
    dma = pltpu.SemaphoreType.DMA
    vm = pltpu.VMEM
    wide = vm((groups, rows, LANES), F32)
    padded = vm((groups, rows + PAD, LANES), F32)
    tpad = -(-(tap_count + 1) // 16) * 16
    any_spec = pl.BlockSpec(memory_space=pltpu.HBM)
    vmem_spec = pl.BlockSpec(memory_space=pltpu.VMEM)
    outs = pl.pallas_call(
        functools.partial(kernel, (nsp, ntp, ny, nz, nx, float(chan))),
        out_shape=(
            jax.ShapeDtypeStruct((rows, dt), BF16),
            jax.ShapeDtypeStruct((3, ds, cl), F32),
            jax.ShapeDtypeStruct((tap_count, cl), F32),
            jax.ShapeDtypeStruct((1, cl), F32),
        ),
        in_specs=[any_spec] * 7,
        out_specs=[vmem_spec] * 4,
        scratch_shapes=[
            vm((rows, width), BF16), vm((width, cl), BF16), vm((width, cl), BF16), vm((width, cl), BF16),
            vm((rows, width), BF16),
            vm((tap_count, cl), F32), vm((1, cl), F32),
            wide, wide, wide, padded, wide, wide, padded,
            vm((rows, cl), BF16), vm((rows, 2 * cl), BF16), vm((rows, 2 * cl), BF16),
            vm((nx, 2, dt, cl), BF16),
            vm((2, 8, LANES), F32), vm((ntp - 1, 2, 8, LANES), F32),
            vm((2, 8, LANES), F32), vm((ntp - 1, 2, 8, LANES), F32),
            vm((rows, LANES), F32), vm((rows, LANES), F32),
            vm((3, nsp, ds, cl), BF16), vm((3, ny - 1, nz, ds, cl), BF16),
            vm((3, nz - 1, ds, cl), BF16), vm((3, nz + 1, ds, cl), BF16),
            vm((nz, ny, late, cl), BF16), vm((nz + 1, ny, late, cl), BF16),
            vm((ny - 1, late, cl), BF16), vm((ny, late, cl), F32),
            vm((nx - 1, nrc, MATMUL_ROWS, dt), BF16), vm((nx - 1, nrc, MATMUL_ROWS, dt), BF16),
            vm((tpad, cl), F32), vm((tpad, cl), BF16), vm((ny - 1, tpad, cl), BF16),
            vm((tpad, cl), BF16), vm((nz - 1, tpad, cl), BF16),
            dma((6 + nrc,)), dma((4,)),
            dma((2, ntp - 1)), dma((2, ntp - 1)),
            dma((nx, 2)), dma((nx, 2)),
            dma((nrc,)), dma((nrc,)),
            dma((nx - 1, nrc)), dma((nx - 1, nrc)),
            dma((3, ny - 1, nz)), dma((3, ny - 1, nz)),
            dma((3, nz - 1)), dma((3, nz + 1)),
            dma((nz - 1,)), dma((nz + 1,)), dma((ny - 1,)), dma((ny - 1,)),
            dma((ny - 1,)), dma((ny - 1,)),
            dma((nz - 1,)), dma((nz - 1,)),
        ],
        compiler_params=pltpu.CompilerParams(
            collective_id=0, has_side_effects=True, vmem_limit_bytes=46 * 1000 * 1000),
    )(*[pltpu.with_memory_space_constraint(a, pltpu.HBM) for a in (
        block_input, value_proj, gate_proj, conv_taps, norm_gain.reshape(1, cl), out_proj, grad_output)])
    outs = pl.pallas_call(
        hand_out,
        out_shape=(
            jax.ShapeDtypeStruct((rows, dt), BF16),
            jax.ShapeDtypeStruct((ds, cl), F32),
            jax.ShapeDtypeStruct((ds, cl), F32),
            jax.ShapeDtypeStruct((ds, cl), F32),
            jax.ShapeDtypeStruct((tap_count, cl), F32),
            jax.ShapeDtypeStruct((1, cl), F32),
        ),
        in_specs=[vmem_spec] * 4,
        out_specs=[any_spec] * 6,
        scratch_shapes=[dma((6,))],
        compiler_params=pltpu.CompilerParams(vmem_limit_bytes=8 * 1000 * 1000),
    )(*outs)
    return outs[:5] + (outs[5].reshape(cl),)


def solution(mesh):
    return jax.shard_map(
        functools.partial(shards, mesh.shape["sp"], mesh.shape["tp"]),
        mesh=mesh,
        in_specs=(
            P("sp", None),
            P(None, "tp"),
            P(None, "tp"),
            P(None, "tp"),
            P("tp"),
            P(None, "tp"),
            P("sp", None),
        ),
        out_specs=(
            P("sp", "tp"),
            P("sp", "tp"),
            P("sp", "tp"),
            P("sp", "tp"),
            P(None, "tp"),
            P("tp"),
        ),
        check_vma=False,
    )
```

```python
import functools

import jax
import jax.numpy as jnp
from jax import lax
from jax.experimental import pallas as pl
from jax.experimental.pallas import tpu as pltpu
from jax.sharding import PartitionSpec as P

NORM_FLOOR = 0.1
LANES = 128
ROW_BLOCK = 128
MATMUL_ROWS = 256
PAD = 32
EARLY_FROM = 4
F32 = jnp.float32
BF16 = jnp.bfloat16
MESH = pl.DeviceIdType.MESH


def dot_nt(a, b):
    return lax.dot_general(a, b, (((1,), (1,)), ((), ())), preferred_element_type=F32)


def dot_tn(a, b):
    return lax.dot_general(a, b, (((0,), (0,)), ((), ())), preferred_element_type=F32)


def kernel(cfg, bi_hbm, wv_hbm, wg_hbm, taps_hbm, gain_hbm, wo_hbm, go_hbm,
           ig_ref, wgrad_ref, tgrad_ref, gaingrad_ref,
           bi, wv, wg, wo, go, taps_ref, gain_ref, val, sg, slope, hist, nrm, nsl, fut, act, sl, psl, pw,
           st1, st1r, st2, st2r, spa, spb, gb, yb, zb, zin, eb, ein, ey, ef,
           xs, xr, tg, tgb, tgy, tgz, tgzr,
           ld_sem, halo_sem, st_send, st_recv, pw_send, pw_recv, sl_send, sl_recv,
           x_send, x_recv, y_send, y_recv, z_send, z_recv, e_send, e_recv, ey_send, ey_recv, ty_send, ty_recv, tz_send, tz_recv):
    nsp, ntp, ny, nz, nx, chan = cfg
    rows, width = bi.shape
    cl = wv.shape[1]
    groups = cl // LANES
    tap_count = taps_ref.shape[0]
    nb = rows // ROW_BLOCK
    vpb = ROW_BLOCK // 8
    nrc = rows // MATMUL_ROWS
    ds = width // nsp
    dt = width // ntp
    sp = lax.axis_index("sp")
    tp = lax.axis_index("tp")
    z = sp // ny
    y = sp % ny
    x = tp // 2
    core = tp % 2

    def wrap(v, n):
        return lax.rem(v, n)

    loads = {}

    def load(name, src, dst, i):
        c = pltpu.make_async_copy(src, dst, ld_sem.at[i])
        c.start()
        loads[name] = c

    load("wv", wv_hbm, wv, 0)
    load("wg", wg_hbm, wg, 1)
    for n, i in enumerate(reversed(range(nrc))):
        s = pl.ds(i * MATMUL_ROWS, MATMUL_ROWS)
        load("bi%d" % i, bi_hbm.at[s], bi.at[s], 2 + n)
    load("taps", taps_hbm, taps_ref, 2 + nrc)
    load("gain", gain_hbm, gain_ref, 3 + nrc)
    load("wo", wo_hbm, wo, 4 + nrc)
    load("go", go_hbm, go, 5 + nrc)

    barrier = pltpu.get_barrier_semaphore()
    for o in range(1, nsp):
        pl.semaphore_signal(barrier, inc=1, device_id={"sp": wrap(sp + o, nsp)}, device_id_type=MESH)
    for o in range(1, ntp):
        pl.semaphore_signal(barrier, inc=1, device_id={"tp": wrap(tp + o, ntp)}, device_id_type=MESH)

    def remote(src, dst, ssem, rsem, dev):
        return pltpu.make_async_remote_copy(
            src_ref=src, dst_ref=dst, send_sem=ssem, recv_sem=rsem, device_id=dev, device_id_type=MESH)

    def glu(i):
        r = i * MATMUL_ROWS
        a = bi[r:r + MATMUL_ROWS, :]
        v = jnp.dot(a, wv[...], preferred_element_type=F32)
        s = jax.nn.sigmoid(jnp.dot(a, wg[...], preferred_element_type=F32))
        m = (v * s).astype(BF16).astype(F32)
        for g in range(groups):
            c = slice(g * LANES, (g + 1) * LANES)
            val[g, r:r + MATMUL_ROWS, :] = v[:, c]
            sg[g, r:r + MATMUL_ROWS, :] = s[:, c]
            hist[g, PAD + r:PAD + r + MATMUL_ROWS, :] = m[:, c]

    halo = remote(hist.at[:, pl.ds(rows, PAD), :], hist.at[:, pl.ds(0, PAD), :],
                  halo_sem.at[0], halo_sem.at[1], {"sp": jnp.minimum(sp + 1, nsp - 1)})
    back = remote(fut.at[:, pl.ds(0, PAD), :], fut.at[:, pl.ds(rows, PAD), :],
                  halo_sem.at[2], halo_sem.at[3], {"sp": jnp.maximum(sp - 1, 0)})
    has_next = sp < nsp - 1
    has_prev = sp > 0

    @pl.when(jnp.logical_not(has_prev))
    def _():
        hist[:, 0:PAD, :] = jnp.zeros((groups, PAD, LANES), F32)

    @pl.when(jnp.logical_not(has_next))
    def _():
        fut[:, rows:rows + PAD, :] = jnp.zeros((groups, PAD, LANES), F32)

    lane = lax.broadcasted_iota(jnp.int32, (8, LANES), 1)

    def pack(packed, red, b):
        for i in range(vpb):
            packed = jnp.where(lane == b * vpb + i, red[8 * i:8 * i + 8], packed)
        return packed

    ahead = (lax.broadcasted_iota(jnp.int32, (ROW_BLOCK, LANES), 1)
             - lax.broadcasted_iota(jnp.int32, (ROW_BLOCK, LANES), 0) // 8)
    ones = jnp.ones((3 * LANES, LANES), BF16)

    def spread(packed, dst):
        high = packed.astype(BF16).astype(F32)
        rest = packed - high
        mid = rest.astype(BF16).astype(F32)
        parts = [jnp.concatenate([p] * vpb, axis=0) for p in (high, mid, rest - mid)]
        for b in range(nb):
            own = ahead == b * vpb
            t = jnp.concatenate([jnp.where(own, p, 0.0).astype(BF16) for p in parts], axis=1)
            dst[b * ROW_BLOCK:(b + 1) * ROW_BLOCK, :] = jnp.dot(t, ones, preferred_element_type=F32)

    def tap(k, g):
        return taps_ref[k:k + 1, g * LANES:(g + 1) * LANES]

    def conv_block(b, carry):
        psum, psq = carry
        s = q = None
        for g in range(groups):
            acc = jnp.zeros((ROW_BLOCK, LANES), F32)
            for k in range(tap_count):
                acc = acc + tap(k, g) * hist[g, pl.ds(b * ROW_BLOCK + (PAD - k), ROW_BLOCK), :]
            nrm[g, pl.ds(pl.multiple_of(b * ROW_BLOCK, ROW_BLOCK), ROW_BLOCK), :] = acc
            s = acc if s is None else s + acc
            q = acc * acc if q is None else q + acc * acc
        return (pack(psum, jnp.sum(s, axis=1, keepdims=True), b),
                pack(psq, jnp.sum(q, axis=1, keepdims=True), b))

    zero = jnp.zeros((8, LANES), F32)
    loads["wv"].wait()
    loads["wg"].wait()
    partner = {"tp": 2 * x + 1 - core}
    pws = []
    bpc = MATMUL_ROWS // ROW_BLOCK
    carry = (zero, zero)
    for n, i in enumerate(reversed(range(nrc))):
        if n == 0:
            loads["bi%d" % i].wait()
        else:
            for b in reversed(range(max(i * bpc + bpc + 1, 0), min(i * bpc + 2 * bpc + 1, nb))):
                carry = conv_block(b, carry)
        glu(i)
        if n == 0:
            loads["taps"].wait()
            loads["gain"].wait()
            for j in reversed(range(nrc - 1)):
                loads["bi%d" % j].wait()
        if n == 1:
            pl.semaphore_wait(barrier, nsp + ntp - 2)

            @pl.when(has_next)
            def _():
                halo.start()

            for xx in range(nx):
                for j, w in enumerate((wv, wg)):
                    first = pl.multiple_of((2 * xx + 1 - core) * dt, dt)
                    c = remote(w.at[pl.ds(first, dt), :], pw.at[xx, j], pw_send.at[xx, j], pw_recv.at[xx, j], partner)
                    c.start()
                    pws.append(c)

    for b in reversed(range(1, bpc + 1)):
        carry = conv_block(b, carry)

    @pl.when(has_prev)
    def _():
        halo.wait_recv()

    psum, psq = conv_block(0, carry)
    st1[0] = psum
    st1[1] = psq

    def share(which, src, dst):
        out = []
        for o in range(1, ntp):
            c = remote(src, dst.at[o - 1], st_send.at[which, o - 1], st_recv.at[which, o - 1],
                       {"tp": wrap(tp + o, ntp)})
            c.start()
            out.append(c)
        return out

    st_copies = share(0, st1, st1r)

    loads["wo"].wait()
    loads["go"].wait()
    for i in range(nrc):
        r = i * MATMUL_ROWS
        t = jnp.dot(go[r:r + MATMUL_ROWS, :], wo[...], preferred_element_type=F32)
        for g in range(groups):
            slope[g, r:r + MATMUL_ROWS, :] = t[:, g * LANES:(g + 1) * LANES]

    for c in st_copies:
        c.wait()
    tsum, tsq = st1[0], st1[1]
    for o in range(ntp - 1):
        tsum = tsum + st1r[o, 0]
        tsq = tsq + st1r[o, 1]
    center = tsum / chan
    inverse = lax.rsqrt(tsq / chan - center * center + NORM_FLOOR)

    spread(center, spa)
    spread(inverse, spb)

    def norm_block(b, carry):
        psum, pcross, gacc = carry
        r = pl.ds(pl.multiple_of(b * ROW_BLOCK, ROW_BLOCK), ROW_BLOCK)
        cen = spa[r, :]
        inv = spb[r, :]
        s = q = None
        gout_acc = []
        for g in range(groups):
            gain = gain_ref[:, g * LANES:(g + 1) * LANES]
            normed = (nrm[g, r, :] - cen) * inv
            scaled = normed * gain
            squash = jax.nn.sigmoid(scaled)
            act[r, g * LANES:(g + 1) * LANES] = (scaled * squash).astype(BF16)
            pre = slope[g, r, :] * squash * (1.0 + scaled * (1.0 - squash))
            pn = pre * normed
            tot = gacc[g]
            for i in range(vpb):
                tot = tot + pn[8 * i:8 * i + 8]
            gout_acc.append(tot)
            ns = pre * gain
            nrm[g, r, :] = normed
            nsl[g, r, :] = ns * inv
            cross = ns * normed
            s = ns if s is None else s + ns
            q = cross if q is None else q + cross
        return (pack(psum, jnp.sum(s, axis=1, keepdims=True), b),
                pack(pcross, jnp.sum(q, axis=1, keepdims=True), b), tuple(gout_acc))

    psum, pcross, gacc = lax.fori_loop(0, nb, norm_block, (zero, zero, (zero,) * groups))
    st2[0] = psum
    st2[1] = pcross
    st_copies = share(1, st2, st2r)

    per = max(1, min(256, width) // ds)
    low = z < nz // 2
    reach = jnp.where(low, nz - 1 - z, z)

    def plane(u):
        if u == nz - 1:
            return z
        up = jnp.where(low, nz - 1 - u, u)
        down = jnp.where(low, u - reach, nz - 1 - (u - reach))
        return jnp.where(u < reach, up, down)

    peers = [(u, r) for u in range(nz) for r in range(1, ny)]

    half = ds * EARLY_FROM // 8
    share_rows = (ds, ds, half)
    y_copies = {}
    for which in range(3):
        for o, r in peers:
            yy = wrap(y + r, ny)
            rs = pl.ds(0, share_rows[which])
            y_copies[which, o, r] = remote(gb.at[which, plane(o) * ny + yy, rs], yb.at[which, r - 1, o, rs],
                                           y_send.at[which, r - 1, o], y_recv.at[which, r - 1, o],
                                           {"sp": z * ny + yy})

    def y_start(which, o):
        for r in range(1, ny):
            y_copies[which, o, r].start()

    def weight_chunk(src, right, first, count, chunk, between=None):
        cols = pl.ds(pl.multiple_of(chunk * per * ds, per * ds), per * ds)
        if between is None:
            t = dot_tn(src[:, cols], right[...])
        else:
            t = None
            for k in range(nrc):
                rs = pl.ds(k * MATMUL_ROWS, MATMUL_ROWS)
                d = dot_tn(src[rs, cols], right[rs, :])
                t = d if t is None else t + d
                between(k)
        t = t.astype(BF16)
        for j in range(per):
            for n in range(count):
                gb[first + n, chunk * per + j] = t[j * ds:(j + 1) * ds, n * cl:(n + 1) * cl]

    def weight_peer(src, right, first, count, o, between=None):
        if per == 1:
            for r in range(1, ny):
                weight_chunk(src, right, first, count, plane(o) * ny + wrap(y + r, ny), between if r == 1 else None)
            between = None
        elif o == 0:
            for chunk in range(nsp // per):
                weight_chunk(src, right, first, count, chunk)
        if between is not None:
            for k in range(nrc):
                between(k)

    def weight_own(src, right, first, count, o, between=None):
        if per == 1:
            weight_chunk(src, right, first, count, plane(o) * ny + y, between)
        elif between is not None:
            for k in range(nrc):
                between(k)

    def y_sum(which, u):
        n = share_rows[which]
        t = gb[which, plane(u) * ny + y, 0:n].astype(F32)
        for r in range(1, ny):
            y_copies[which, u, r].wait()
            t = t + yb[which, r - 1, u, 0:n].astype(F32)
        return t

    def chain_in(which, slot):
        rs = pl.ds(0, share_rows[which])
        return remote(zin.at[which, slot, rs], zin.at[which, slot, rs], z_send.at[which, 0], z_recv.at[which, slot],
                      {"sp": wrap(z + 1, nz) * ny + y})

    edge = jnp.logical_or(z == 0, z == nz - 1)

    def chain_to(u):
        p = plane(u)
        return jnp.where(p == z - 1, nz, p), {"sp": jnp.where(p > z, z + 1, z - 1) * ny + y}

    def chain_copy(which, u):
        slot, dev = chain_to(u)
        rs = pl.ds(0, share_rows[which])
        return remote(zb.at[which, u, rs], zin.at[which, slot, rs], z_send.at[which, u], z_recv.at[which, slot], dev)

    def edge_step(which, u):
        @pl.when(edge)
        def _():
            zb[which, u, 0:share_rows[which]] = y_sum(which, u).astype(BF16)
            chain_copy(which, u).start()

    def middle_step(which, u):
        @pl.when(jnp.logical_not(edge))
        def _():
            n = share_rows[which]
            t = y_sum(which, u)
            chain_in(which, plane(u)).wait_recv()
            zb[which, u, 0:n] = (t + zin[which, plane(u), 0:n].astype(F32)).astype(BF16)
            chain_copy(which, u).start()

    def final_sum(which):
        n = share_rows[which]
        wgrad_ref[which, 0:n] = y_sum(which, nz - 1)

        @pl.when(z > 0)
        def _():
            chain_in(which, z).wait_recv()
            wgrad_ref[which, 0:n] = wgrad_ref[which, 0:n] + zin[which, z, 0:n].astype(F32)

        @pl.when(z < nz - 1)
        def _():
            chain_in(which, nz).wait_recv()
            wgrad_ref[which, 0:n] = wgrad_ref[which, 0:n] + zin[which, nz, 0:n].astype(F32)

    def early_in(slot):
        return remote(ein.at[slot], ein.at[slot], e_send.at[0], e_recv.at[slot], {"sp": wrap(z + 1, nz) * ny + y})

    def early_copy(u, src):
        slot, dev = chain_to(u)
        return remote(src, ein.at[slot], e_send.at[u], e_recv.at[slot], dev)

    def early_own(p):
        return gb[2, pl.ds(p * ny, ny), half:ds].astype(F32)

    def early_edge(u):
        @pl.when(edge)
        def _():
            early_copy(u, gb.at[2, pl.ds(plane(u) * ny, ny), pl.ds(half, ds - half)]).start()

    def early_middle(u):
        @pl.when(jnp.logical_not(edge))
        def _():
            early_in(plane(u)).wait_recv()
            eb[u] = (early_own(plane(u)) + ein[plane(u)].astype(F32)).astype(BF16)
            early_copy(u, eb.at[u]).start()

    early_y = []
    for r in range(1, ny):
        yy = wrap(y + r, ny)
        early_y.append(remote(eb.at[nz - 1, yy], ey.at[r - 1], ey_send.at[r - 1], ey_recv.at[r - 1],
                              {"sp": z * ny + yy}))

    def early_turn():
        ef[...] = early_own(z)

        @pl.when(z > 0)
        def _():
            early_in(z).wait_recv()
            ef[...] = ef[...] + ein[z].astype(F32)

        @pl.when(z < nz - 1)
        def _():
            early_in(nz).wait_recv()
            ef[...] = ef[...] + ein[nz].astype(F32)

        eb[nz - 1] = ef[...].astype(BF16)
        for c in early_y:
            c.start()

    def early_final():
        t = ef[y]
        for r in range(1, ny):
            early_y[r - 1].wait()
            t = t + ey[r - 1].astype(F32)
        wgrad_ref[2, half:ds] = t

    weight_peer(go, act, 2, 1, 0)
    y_start(2, 0)
    weight_own(go, act, 2, 1, 0)
    early_edge(0)
    weight_peer(go, act, 2, 1, 1)
    y_start(2, 1)
    weight_own(go, act, 2, 1, 1)
    for o in range(2, nz - 1):
        weight_peer(go, act, 2, 1, o)

    for c in st_copies:
        c.wait()
    tsum, tcross = st2[0], st2[1]
    for o in range(ntp - 1):
        tsum = tsum + st2r[o, 0]
        tcross = tcross + st2r[o, 1]
    tsum = tsum / chan * inverse
    tcross = tcross / chan * inverse

    spread(tsum, spa)
    spread(tcross, spb)

    def slope_block(b, c):
        r = pl.ds(pl.multiple_of(b * ROW_BLOCK, ROW_BLOCK), ROW_BLOCK)
        ss = spa[r, :]
        cs = spb[r, :]
        for g in range(groups):
            fut[g, r, :] = nsl[g, r, :] - ss - nrm[g, r, :] * cs
        return c

    slope_block(0, 0)

    @pl.when(has_prev)
    def _():
        back.start()

    for o in range(2, nz - 1):
        y_start(2, o)
    early_edge(1)

    lax.fori_loop(1, nb, slope_block, 0)

    def adjoint_block(b, only=None):
        r = pl.ds(pl.multiple_of(b * ROW_BLOCK, ROW_BLOCK), ROW_BLOCK)
        for g in range(groups) if only is None else only:
            acc = jnp.zeros((ROW_BLOCK, LANES), F32)
            for k in range(tap_count):
                acc = acc + tap(k, g) * fut[g, pl.ds(b * ROW_BLOCK + k, ROW_BLOCK), :]
            s = sg[g, r, :]
            t = acc * s
            sl[r, g * LANES:(g + 1) * LANES] = t.astype(BF16)
            sl[r, cl + g * LANES:cl + (g + 1) * LANES] = (t * val[g, r, :] * (1.0 - s)).astype(BF16)

    def input_part(i, xx):
        r = slice(i * MATMUL_ROWS, (i + 1) * MATMUL_ROWS)
        blk = pl.ds(pl.multiple_of((2 * xx + core) * dt, dt), dt)
        t = dot_nt(sl[r, 0:cl], wv[blk, :]) + dot_nt(sl[r, cl:2 * cl], wg[blk, :])
        return t + dot_nt(psl[r, 0:cl], pw[xx, 0]) + dot_nt(psl[r, cl:2 * cl], pw[xx, 1])

    xc = []

    def input_send(i):
        for o in range(1, nx):
            xx = wrap(x + o, nx)
            xs[o - 1, i] = input_part(i, xx).astype(BF16)
            c = remote(xs.at[o - 1, i], xr.at[o - 1, i], x_send.at[o - 1, i], x_recv.at[o - 1, i],
                       {"tp": 2 * xx + core})
            c.start()
            xc.append(c)

    for c in pws:
        c.wait()
    slc = []
    for i in range(nrc):
        if i == 2:
            slc[0].wait()
        todo = [(b, g) for b in range(i * bpc, nb - 1 if i == nrc - 1 else (i + 1) * bpc) for g in range(groups)]

        def between(k, todo=todo):
            for b, g in todo[k * len(todo) // nrc:(k + 1) * len(todo) // nrc]:
                adjoint_block(b, (g,))

        if not (i == 0 or i == 1):
            for k in range(nrc):
                between(k)
        if i == 2:
            input_send(0)
        if i == 0:
            for o in range(2, nz - 1):
                weight_own(go, act, 2, 1, o, between if o == 2 else None)
                early_edge(o)
        if i == 1:
            weight_peer(go, act, 2, 1, nz - 1, between)
            y_start(2, nz - 1)
        if i == nrc - 1:
            early_middle(0)

            @pl.when(has_next)
            def _():
                back.wait_recv()

            adjoint_block(nb - 1)
        s = pl.ds(i * MATMUL_ROWS, MATMUL_ROWS)
        c = remote(sl.at[s], psl.at[s], sl_send.at[i], sl_recv.at[i], partner)
        c.start()
        slc.append(c)

    for o in range(nz):
        weight_peer(bi, sl, 0, 2, o)
        if o < nz - 1:
            y_start(0, o)
            y_start(1, o)

    for u in range(nz - 1):
        edge_step(2, u)
    for i in range(1, nrc - 1):
        slc[i].wait()
        input_send(i)
    early_middle(1)
    weight_own(go, act, 2, 1, nz - 1)
    for o in range(nz):
        weight_own(bi, sl, 0, 2, o)
    edge_step(0, 0)
    slc[nrc - 1].wait()
    input_send(nrc - 1)

    step = 4
    def taps_part(g):
        def tap_block(b, accs):
            r = b * 8 * step
            f = fut[g, pl.ds(pl.multiple_of(r, 8 * step), 8 * step), :]
            out = []
            for k in range(tap_count):
                p = f * hist[g, pl.ds(r + (PAD - k), 8 * step), :]
                t = accs[k]
                for i in range(step):
                    t = t + p[8 * i:8 * i + 8]
                out.append(t)
            return tuple(out)

        accs = lax.fori_loop(0, rows // (8 * step), tap_block, (zero,) * tap_count)
        for k in range(tap_count):
            tg[k:k + 1, g * LANES:(g + 1) * LANES] = jnp.sum(accs[k], axis=0, keepdims=True)
        tg[tap_count:tap_count + 1, g * LANES:(g + 1) * LANES] = jnp.sum(gacc[g], axis=0, keepdims=True)

    def input_own(i):
        t = input_part(i, x)
        for o in range(1, nx):
            xc[i * (nx - 1) + o - 1].wait()
            t = t + xr[o - 1, i].astype(F32)
        ig_ref[i * MATMUL_ROWS:(i + 1) * MATMUL_ROWS, :] = t.astype(BF16)

    queue = [(which, u) for u in range(nz - 1) for which in range(2)]
    middle = queue[:-4] + [queue[-2], queue[-4], queue[-1], queue[-3]]

    taps_part(0)
    for u in range(2, nz - 1):
        early_middle(u)
    middle_step(2, 0)
    edge_step(*queue[1])
    for g in range(1, groups):
        taps_part(g)
    tgb[...] = tg[...].astype(BF16)
    tzc = []
    for o in range(1, nz):
        c = remote(tgb, tgzr.at[o - 1], tz_send.at[o - 1], tz_recv.at[o - 1], {"sp": wrap(z + o, nz) * ny + y})
        c.start()
        tzc.append(c)

    for u in range(1, nz - 2):
        middle_step(2, u)
    edge_step(*queue[2])
    middle_step(2, nz - 2)
    middle_step(*middle[0])
    early_turn()
    y_start(0, nz - 1)
    edge_step(*queue[3])
    tyc = []
    done = 0
    for n in range(1, len(queue)):
        middle_step(*middle[n])
        if n == 1:
            input_own(done)
            done += 1
        if n + 3 < len(queue):
            edge_step(*queue[n + 3])
        if n == 2:
            t = tgb[...].astype(F32)
            for o in range(1, nz):
                tzc[o - 1].wait()
                t = t + tgzr[o - 1].astype(F32)
            tgz[...] = t.astype(BF16)
            for r in range(1, ny):
                c = remote(tgz, tgy.at[r - 1], ty_send.at[r - 1], ty_recv.at[r - 1],
                           {"sp": z * ny + wrap(y + r, ny)})
                c.start()
                tyc.append(c)
            y_start(1, nz - 1)
        if n > 2 and done < nrc - 1:
            input_own(done)
            done += 1
    for i in range(done, nrc):
        input_own(i)
    early_final()
    final_sum(2)
    t = tgz[...].astype(F32)
    for r in range(1, ny):
        tyc[r - 1].wait()
        t = t + tgy[r - 1].astype(F32)
    tgrad_ref[...] = t[0:tap_count]
    gaingrad_ref[...] = t[tap_count:tap_count + 1]
    final_sum(0)
    final_sum(1)
    for u in range(nz - 1):
        early_copy(u, eb.at[u]).wait_send()
        for which in range(3):
            chain_copy(which, u).wait_send()

    @pl.when(has_next)
    def _():
        halo.wait_send()

    @pl.when(has_prev)
    def _():
        back.wait_send()


def hand_out(ig, wgrad, taps, gain, ig_ref, vgrad_ref, ggrad_ref, ograd_ref, tgrad_ref, gaingrad_ref, out_sem):
    moves = [(wgrad.at[i], ref) for i, ref in enumerate((vgrad_ref, ggrad_ref, ograd_ref))]
    moves += [(ig, ig_ref), (taps, tgrad_ref), (gain, gaingrad_ref)]
    copies = [pltpu.make_async_copy(src, dst, out_sem.at[i]) for i, (src, dst) in enumerate(moves)]
    for c in copies:
        c.start()
    for c in copies:
        c.wait()


def shards(nsp, ntp, block_input, value_proj, gate_proj, conv_taps, norm_gain, out_proj, grad_output):
    rows, width = block_input.shape
    cl = value_proj.shape[1]
    chan = cl * ntp
    nx = ntp // 2
    ny = nx
    nz = nsp // ny
    groups = cl // LANES
    ds = width // nsp
    late = ds - ds * EARLY_FROM // 8
    dt = width // ntp
    nrc = rows // MATMUL_ROWS
    tap_count = conv_taps.shape[0]
    dma = pltpu.SemaphoreType.DMA
    vm = pltpu.VMEM
    wide = vm((groups, rows, LANES), F32)
    padded = vm((groups, rows + PAD, LANES), F32)
    tpad = -(-(tap_count + 1) // 16) * 16
    any_spec = pl.BlockSpec(memory_space=pltpu.HBM)
    vmem_spec = pl.BlockSpec(memory_space=pltpu.VMEM)
    outs = pl.pallas_call(
        functools.partial(kernel, (nsp, ntp, ny, nz, nx, float(chan))),
        out_shape=(
            jax.ShapeDtypeStruct((rows, dt), BF16),
            jax.ShapeDtypeStruct((3, ds, cl), F32),
            jax.ShapeDtypeStruct((tap_count, cl), F32),
            jax.ShapeDtypeStruct((1, cl), F32),
        ),
        in_specs=[any_spec] * 7,
        out_specs=[vmem_spec] * 4,
        scratch_shapes=[
            vm((rows, width), BF16), vm((width, cl), BF16), vm((width, cl), BF16), vm((width, cl), BF16),
            vm((rows, width), BF16),
            vm((tap_count, cl), F32), vm((1, cl), F32),
            wide, wide, wide, padded, wide, wide, padded,
            vm((rows, cl), BF16), vm((rows, 2 * cl), BF16), vm((rows, 2 * cl), BF16),
            vm((nx, 2, dt, cl), BF16),
            vm((2, 8, LANES), F32), vm((ntp - 1, 2, 8, LANES), F32),
            vm((2, 8, LANES), F32), vm((ntp - 1, 2, 8, LANES), F32),
            vm((rows, LANES), F32), vm((rows, LANES), F32),
            vm((3, nsp, ds, cl), BF16), vm((3, ny - 1, nz, ds, cl), BF16),
            vm((3, nz - 1, ds, cl), BF16), vm((3, nz + 1, ds, cl), BF16),
            vm((nz, ny, late, cl), BF16), vm((nz + 1, ny, late, cl), BF16),
            vm((ny - 1, late, cl), BF16), vm((ny, late, cl), F32),
            vm((nx - 1, nrc, MATMUL_ROWS, dt), BF16), vm((nx - 1, nrc, MATMUL_ROWS, dt), BF16),
            vm((tpad, cl), F32), vm((tpad, cl), BF16), vm((ny - 1, tpad, cl), BF16),
            vm((tpad, cl), BF16), vm((nz - 1, tpad, cl), BF16),
            dma((6 + nrc,)), dma((4,)),
            dma((2, ntp - 1)), dma((2, ntp - 1)),
            dma((nx, 2)), dma((nx, 2)),
            dma((nrc,)), dma((nrc,)),
            dma((nx - 1, nrc)), dma((nx - 1, nrc)),
            dma((3, ny - 1, nz)), dma((3, ny - 1, nz)),
            dma((3, nz - 1)), dma((3, nz + 1)),
            dma((nz - 1,)), dma((nz + 1,)), dma((ny - 1,)), dma((ny - 1,)),
            dma((ny - 1,)), dma((ny - 1,)),
            dma((nz - 1,)), dma((nz - 1,)),
        ],
        compiler_params=pltpu.CompilerParams(
            collective_id=0, has_side_effects=True, vmem_limit_bytes=46 * 1000 * 1000),
    )(*[pltpu.with_memory_space_constraint(a, pltpu.HBM) for a in (
        block_input, value_proj, gate_proj, conv_taps, norm_gain.reshape(1, cl), out_proj, grad_output)])
    outs = pl.pallas_call(
        hand_out,
        out_shape=(
            jax.ShapeDtypeStruct((rows, dt), BF16),
            jax.ShapeDtypeStruct((ds, cl), F32),
            jax.ShapeDtypeStruct((ds, cl), F32),
            jax.ShapeDtypeStruct((ds, cl), F32),
            jax.ShapeDtypeStruct((tap_count, cl), F32),
            jax.ShapeDtypeStruct((1, cl), F32),
        ),
        in_specs=[vmem_spec] * 4,
        out_specs=[any_spec] * 6,
        scratch_shapes=[dma((6,))],
        compiler_params=pltpu.CompilerParams(vmem_limit_bytes=8 * 1000 * 1000),
    )(*outs)
    return outs[:5] + (outs[5].reshape(cl),)


def solution(mesh):
    return jax.shard_map(
        functools.partial(shards, mesh.shape["sp"], mesh.shape["tp"]),
        mesh=mesh,
        in_specs=(
            P("sp", None),
            P(None, "tp"),
            P(None, "tp"),
            P(None, "tp"),
            P("tp"),
            P(None, "tp"),
            P("sp", None),
        ),
        out_specs=(
            P("sp", "tp"),
            P("sp", "tp"),
            P("sp", "tp"),
            P("sp", "tp"),
            P(None, "tp"),
            P("tp"),
        ),
        check_vma=False,
    )
```
